32 devices in a mesh: sp: 16 (over z, y, x), tp: 2 (over core).
Axes of the slice: x: 2, y: 2, z: 4, core: 2. Of those that a mesh axis runs over, the one named last changes fastest.
Arguments:
- residual: bfloat16 [2048, 2048], P('sp'), may hold values from -6 to 6
- query_first: bfloat16 [2048, 8, 128], P('sp', 'tp'), may hold values from -6.5 to 6.5
- key_first: bfloat16 [2048, 8, 128], P('sp', 'tp'), may hold values from -6.5 to 6.5
- value_first: bfloat16 [2048, 8, 128], P('sp', 'tp'), may hold values from -6 to 6
- query_second: bfloat16 [2048, 8, 64], P('sp', 'tp'), may hold values from -6.5 to 6.5
- key_second: bfloat16 [2048, 8, 64], P('sp', 'tp'), may hold values from -6.5 to 6.5
- value_second: bfloat16 [2048, 8, 64], P('sp', 'tp'), may hold values from -6 to 6
- balance_first: float32 [8], P('tp'), may hold values from 0.3 to 0.8
- balance_second: float32 [8], P('tp'), may hold values from 0.3 to 0.8
- head_gain_first: float32 [128], replicated, may hold values from 0.1 to 1.9
- head_gain_second: float32 [64], replicated, may hold values from 0.1 to 1.9
- out_first: bfloat16 [1024, 2048], P('tp'), may hold values from -0.15625 to 0.15625
- out_second: bfloat16 [512, 2048], P('tp'), may hold values from -0.15625 to 0.15625
- mlp_gain: float32 [2048], replicated, may hold values from 0.1 to 1.9
- up_weight: bfloat16 [2048, 8192], P('sp', 'tp'), may hold values from -0.125 to 0.125
- down_weight: bfloat16 [2048, 8192], P('sp', 'tp'), may hold values from -0.0625 to 0.0625
Outputs:
- layer_out: bfloat16 [2048, 2048], P('sp')
The draws below stay inside these ranges and needn't reach their ends.
All inputs are finite; a program needn't handle non-finite values.
Results may differ from the reference program's by a relative error of at most 0.018.
Values may be sent and summed in bfloat16 or wider, within the bound.
No kernel may reach another device: no remote copies, remote signals or barrier semaphores. Data moves between devices by JAX's collectives and lax.ppermute only.
A program may use at most 128 MiB of HBM per device.

```python
import math
import jax
import jax.numpy as jnp
from jax import lax

D = 2048
FF = 8192
HEADS_A = 8
HEADS_B = 8
DK_A = 64
DV_A = 128
DK_B = 32
DV_B = 64
SEQ = 2048
N_TP = 2


def drawn(key, heads, head_size):
    width = 2 * head_size
    queries = jnp.clip(1.3 * jax.random.normal(jax.random.fold_in(key, 11), (SEQ, heads, width), jnp.float32), -6.5, 6.5)
    keys = jnp.clip(1.3 * jax.random.normal(jax.random.fold_in(key, 12), (SEQ, heads, width), jnp.float32), -6.5, 6.5)
    return (queries, keys)


def draw_query_first(key, part):
    return drawn(jax.random.fold_in(key, 1), HEADS_A, DK_A)[0].astype(jnp.bfloat16)


def draw_key_first(key, part):
    return drawn(jax.random.fold_in(key, 1), HEADS_A, DK_A)[1].astype(jnp.bfloat16)


def draw_query_second(key, part):
    return drawn(jax.random.fold_in(key, 2), HEADS_B, DK_B)[0].astype(jnp.bfloat16)


def draw_key_second(key, part):
    return drawn(jax.random.fold_in(key, 2), HEADS_B, DK_B)[1].astype(jnp.bfloat16)


def block_scale(key, dims, shards, smallest, high):
    loudness = 1.0
    for position, parts in shards:
        draws = jax.random.uniform(jax.random.fold_in(jax.random.fold_in(key, 6), position), (parts,), jnp.float32, smallest / len(shards), high / len(shards))
        loudness = loudness * jnp.repeat(jnp.exp(draws), dims[position] // parts).reshape((-1,) + (1,) * (len(dims) - 1 - position))
    return loudness


def gaussian(rng, shape, spread, limit, split=(), kind=jnp.bfloat16):
    values = spread * jax.random.normal(rng, shape, jnp.float32)
    if split:
        values = values * block_scale(rng, shape, split, -0.22, 0.18)
    return jnp.clip(values, -limit, limit).astype(kind)


def setup_inputs(seed: int = 0) -> dict:
    key_list = jax.random.split(jax.random.key(seed), 17)
    return {
        "residual": gaussian(key_list[0], (SEQ, D), 1.0, 6.0, ((0, 16),)),
        "query_first": draw_query_first(jax.random.fold_in(key_list[16], 71), 0),
        "key_first": draw_key_first(jax.random.fold_in(key_list[16], 71), 0),
        "value_first": gaussian(key_list[3], (SEQ, HEADS_A, DV_A), 1.0, 6.0, ((0, 16), (1, 2))),
        "query_second": draw_query_second(jax.random.fold_in(key_list[16], 71), 0),
        "key_second": draw_key_second(jax.random.fold_in(key_list[16], 71), 0),
        "value_second": gaussian(key_list[6], (SEQ, HEADS_B, DV_B), 1.0, 6.0, ((0, 16), (1, 2))),
        "balance_first": jnp.clip(0.3 + 0.5 * jax.random.uniform(key_list[7], (HEADS_A,), jnp.float32) ** block_scale(key_list[7], (HEADS_A,), ((0, 2),), -0.2, 0.2), 0.3, 0.8),
        "balance_second": jnp.clip(0.3 + 0.5 * jax.random.uniform(key_list[8], (HEADS_B,), jnp.float32) ** block_scale(key_list[8], (HEADS_B,), ((0, 2),), -0.2, 0.2), 0.3, 0.8),
        "head_gain_first": jnp.clip(1.0 + 0.18 * jax.random.normal(key_list[9], (DV_A,), jnp.float32), 0.1, 1.9),
        "head_gain_second": jnp.clip(1.0 + 0.18 * jax.random.normal(key_list[10], (DV_B,), jnp.float32), 0.1, 1.9),
        "out_first": gaussian(key_list[11], (HEADS_A * DV_A, D), (HEADS_A * DV_A + HEADS_B * DV_B) ** -0.5, 0.15625, ((0, 2),)),
        "out_second": gaussian(key_list[12], (HEADS_B * DV_B, D), (HEADS_A * DV_A + HEADS_B * DV_B) ** -0.5, 0.15625, ((0, 2),)),
        "mlp_gain": jnp.clip(1.0 + 0.18 * jax.random.normal(key_list[13], (D,), jnp.float32), 0.1, 1.9),
        "up_weight": gaussian(key_list[14], (D, FF), D ** -0.5, 0.125, ((0, 16), (1, 2))),
        "down_weight": gaussian(key_list[15], (D, FF), FF ** -0.5, 0.0625, ((0, 16), (1, 2))),
    }


EPSILON = 1e-06
HEAD_SCALE = 0.8

def group_heads(queries, keys, values, balance, gain, head_size):
    seq = queries.shape[0]
    heads = queries.shape[1]
    depth = values.shape[2]
    block = math.gcd(256, seq)
    count = seq // block
    query_maps = queries.astype(jnp.float32).reshape(count, block, heads, 2, head_size)
    key_maps = keys.astype(jnp.float32).reshape(seq, heads, 2, head_size)
    value_float = values.astype(jnp.float32)
    columns = jnp.arange(seq, dtype=jnp.int32)
    gain_float = gain.astype(jnp.float32)

    def one_block(args):
        query_block, start = args
        scores = jnp.einsum('qhmd,khmd->hmqk', query_block, key_maps) * head_size ** (-0.5)
        positions = start + jnp.arange(block, dtype=jnp.int32)
        scores = jnp.where(columns[None, :] <= positions[:, None], scores, -jnp.inf)
        probs = jax.nn.softmax(scores, axis=-1)
        mixed = (probs[:, 0] - balance[:, None, None] * probs[:, 1]).astype(jnp.bfloat16)
        mixed = lax.optimization_barrier(mixed).astype(jnp.float32)
        summed = jnp.einsum('hqk,khe->qhe', mixed, value_float)
        power = lax.optimization_barrier(jnp.mean(summed * summed, axis=-1, keepdims=True))
        normed = summed * lax.rsqrt(power + EPSILON) * gain_float * HEAD_SCALE
        return normed.astype(jnp.bfloat16)
    starts = jnp.arange(count, dtype=jnp.int32) * block
    result = lax.map(one_block, (query_maps, starts))
    return result.reshape(seq, heads * depth)

def reference(residual, query_first, key_first, value_first, query_second, key_second, value_second, balance_first, balance_second, head_gain_first, head_gain_second, out_first, out_second, mlp_gain, up_weight, down_weight):
    heads_first = group_heads(query_first, key_first, value_first, balance_first, head_gain_first, DK_A)
    heads_second = group_heads(query_second, key_second, value_second, balance_second, head_gain_second, DK_B)
    seq = residual.shape[0]
    width = residual.shape[1]
    width_first = heads_first.shape[1] // N_TP
    width_second = heads_second.shape[1] // N_TP

    def head_part(number, total):
        offset_first = (number * width_first).astype(jnp.int32)
        offset_second = (number * width_second).astype(jnp.int32)
        part = jnp.dot(lax.dynamic_slice_in_dim(heads_first, offset_first, width_first, 1), lax.dynamic_slice_in_dim(out_first, offset_first, width_first, 0), preferred_element_type=jnp.float32)
        part = part + jnp.dot(lax.dynamic_slice_in_dim(heads_second, offset_second, width_second, 1), lax.dynamic_slice_in_dim(out_second, offset_second, width_second, 0), preferred_element_type=jnp.float32)
        rounded = lax.optimization_barrier(part.astype(jnp.bfloat16))
        return total + rounded.astype(jnp.float32)
    head_total = lax.fori_loop(0, N_TP, head_part, jnp.zeros((seq, width), jnp.float32))
    mixed = (residual.astype(jnp.float32) + head_total).astype(jnp.bfloat16)
    mixed_float = mixed.astype(jnp.float32)
    power = lax.optimization_barrier(jnp.mean(mixed_float * mixed_float, axis=-1, keepdims=True))
    normed = (mixed_float * lax.rsqrt(power + EPSILON) * mlp_gain.astype(jnp.float32)).astype(jnp.bfloat16)
    lifted = jnp.dot(normed, up_weight, preferred_element_type=jnp.float32)
    active = jax.nn.relu(lifted)
    hidden = (active * active).astype(jnp.bfloat16)
    width_hidden = hidden.shape[1] // N_TP

    def down_part(number, total):
        offset = (number * width_hidden).astype(jnp.int32)
        part = lax.dot_general(lax.dynamic_slice_in_dim(hidden, offset, width_hidden, 1), lax.dynamic_slice_in_dim(down_weight, offset, width_hidden, 1), (((1,), (1,)), ((), ())), preferred_element_type=jnp.float32)
        rounded = lax.optimization_barrier(part.astype(jnp.bfloat16))
        return total + rounded.astype(jnp.float32)
    down_total = lax.fori_loop(0, N_TP, down_part, jnp.zeros((seq, width), jnp.float32))
    return (mixed_float + down_total).astype(jnp.bfloat16)
```

```python
import functools
import math

import jax
import jax.numpy as jnp
from jax import lax
from jax.experimental import pallas as pl
from jax.experimental.pallas import tpu as pltpu
from jax.sharding import PartitionSpec as P

DK_A = 64
DK_B = 32


EPSILON = 1e-06
HEAD_SCALE = 0.8


def attend(queries, keys, values, balance, gain, device, head_size):
    tokens = queries.shape[0]
    heads = queries.shape[1]
    seq = keys.shape[0]
    depth = values.shape[2]
    block = math.gcd(512, seq)
    scale = head_size ** (-0.5)
    query_maps = queries.reshape(tokens, heads, 2, head_size)
    key_maps = keys.reshape(seq, heads, 2, head_size)
    first_row = device * tokens
    positions = first_row + jnp.arange(tokens, dtype=jnp.int32)
    needed = (first_row + tokens + block - 1) // block

    def block_scores(number):
        start = number * block
        key_block = lax.dynamic_slice_in_dim(key_maps, start, block, 0)
        scores = (
            jnp.einsum("qhmd,khmd->hmqk", query_maps, key_block, preferred_element_type=jnp.float32)
            * scale
        )
        columns = start + jnp.arange(block, dtype=jnp.int32)
        visible = columns[None, :] <= positions[:, None]
        return (jnp.where(visible, scores, -jnp.inf), start)

    def statistics(number, carry):
        highest, total = carry
        scores, start = block_scores(number)
        fresh = jnp.maximum(highest, jnp.max(scores, axis=-1, keepdims=True))
        total = total * jnp.exp(highest - fresh) + jnp.sum(
            jnp.exp(scores - fresh), axis=-1, keepdims=True
        )
        return (fresh, total)

    start_high = jnp.full((heads, 2, tokens, 1), -jnp.inf, jnp.float32)
    start_total = jnp.zeros((heads, 2, tokens, 1), jnp.float32)
    highest, total = lax.fori_loop(0, needed, statistics, (start_high, start_total))

    def accumulate(number, result):
        scores, start = block_scores(number)
        probs = jnp.exp(scores - highest) / total
        mixed = (probs[:, 0] - balance[:, None, None] * probs[:, 1]).astype(jnp.bfloat16)
        value_block = lax.dynamic_slice_in_dim(values, start, block, 0)
        return result + jnp.einsum(
            "hqk,khe->qhe", mixed, value_block, preferred_element_type=jnp.float32
        )

    summed = lax.fori_loop(0, needed, accumulate, jnp.zeros((tokens, heads, depth), jnp.float32))
    power = jnp.mean(summed * summed, axis=-1, keepdims=True)
    normed = summed * lax.rsqrt(power + EPSILON) * gain * HEAD_SCALE
    return normed.astype(jnp.bfloat16).reshape(tokens, heads * depth)


def body(
    residual,
    query_first,
    key_first,
    value_first,
    query_second,
    key_second,
    value_second,
    balance_first,
    balance_second,
    head_gain_first,
    head_gain_second,
    out_first,
    out_second,
    mlp_gain,
    up_weight,
    down_weight,
):
    device = lax.axis_index("sp")
    keys_first, values_first, keys_second, values_second = (
        lax.all_gather(key_first, "sp", axis=0, tiled=True),
        lax.all_gather(value_first, "sp", axis=0, tiled=True),
        lax.all_gather(key_second, "sp", axis=0, tiled=True),
        lax.all_gather(value_second, "sp", axis=0, tiled=True),
    )
    heads_first = attend(
        query_first, keys_first, values_first, balance_first, head_gain_first, device, DK_A
    )
    heads_second = attend(
        query_second, keys_second, values_second, balance_second, head_gain_second, device, DK_B
    )
    head_term = jnp.dot(heads_first, out_first, preferred_element_type=jnp.float32) + jnp.dot(
        heads_second, out_second, preferred_element_type=jnp.float32
    )
    head_total = lax.psum(head_term.astype(jnp.bfloat16), "tp").astype(jnp.float32)
    mixed = (residual.astype(jnp.float32) + head_total).astype(jnp.bfloat16)
    mixed_float = mixed.astype(jnp.float32)
    power = jnp.mean(mixed_float * mixed_float, axis=-1, keepdims=True)
    normed = (mixed_float * lax.rsqrt(power + EPSILON) * mlp_gain).astype(jnp.bfloat16)
    up_whole, down_whole = (
        lax.all_gather(up_weight, "sp", axis=0, tiled=True),
        lax.all_gather(down_weight, "sp", axis=0, tiled=True),
    )
    lifted = jnp.dot(normed, up_whole, preferred_element_type=jnp.float32)
    active = jax.nn.relu(lifted)
    hidden = (active * active).astype(jnp.bfloat16)
    down_term = lax.dot_general(
        hidden, down_whole, (((1,), (1,)), ((), ())), preferred_element_type=jnp.float32
    )
    added = lax.psum(down_term.astype(jnp.bfloat16), "tp").astype(jnp.float32)
    return (mixed_float + added).astype(jnp.bfloat16)


VMEM = pltpu.VMEM
SMEM = pltpu.SMEM
ROWS = 128


def vmem_specs(count):
    return [pl.BlockSpec(memory_space=VMEM)] * count


def attend_kernel(slots, plane, tokens, index, balance_a, balance_b, gain_a, gain_b, *refs):
    queries, kv_pieces, out = refs[:slots], refs[slots : slots + plane], refs[slots + plane]
    query, keyval, scores = refs[slots + plane + 1 :]
    z, g = index[0], index[1]
    wide = plane * tokens
    for k in range(slots):
        query[z ^ k] = queries[k][...]
        for p in range(plane):
            start = pl.multiple_of(((z ^ k) * plane + (g ^ p)) * tokens, tokens)
            keyval[pl.ds(start, tokens), :] = kv_pieces[p][k]
    lane = lax.broadcasted_iota(jnp.int32, (tokens, 128), 1)
    row = lax.broadcasted_iota(jnp.int32, (2 * tokens, wide), 0) % tokens
    column = lax.broadcasted_iota(jnp.int32, (2 * tokens, wide), 1)
    visible = column <= row + g * tokens

    def group(number, place, size, key_lo, value_lo, balance):
        packed = query[number][:, place : place + 2 * size]
        if 2 * size < 128:
            packed = jnp.concatenate(
                [packed, jnp.zeros((tokens, 128 - 2 * size), packed.dtype)], axis=1
            )
        zero = jnp.zeros_like(packed)
        both = jnp.concatenate(
            [jnp.where(lane < size, packed, zero), jnp.where(lane >= size, packed, zero)], axis=0
        )
        factor = size ** (-0.5) * math.log2(math.e)
        highest = None
        for c in range(number + 1):
            part = lax.dot_general(
                both,
                keyval[c * wide : (c + 1) * wide, key_lo : key_lo + 128],
                (((1,), (1,)), ((), ())),
                preferred_element_type=jnp.float32,
            )
            if c == number:
                part = jnp.where(visible, part, -jnp.inf)
            scores[:, c * wide : (c + 1) * wide] = part
            top = jnp.max(part, axis=1, keepdims=True)
            highest = top if highest is None else jnp.maximum(highest, top)
        total = jnp.zeros((2 * tokens, 1), jnp.float32)
        for c in range(number + 1):
            part = jnp.exp2((scores[:, c * wide : (c + 1) * wide] - highest) * factor)
            scores[:, c * wide : (c + 1) * wide] = part
            total = total + jnp.sum(part, axis=1, keepdims=True)
        share = 1.0 / total
        first, second = share[:tokens], share[tokens:] * balance
        summed = jnp.zeros((tokens, 128), jnp.float32)
        for c in range(number + 1):
            span = slice(c * wide, (c + 1) * wide)
            weights = (scores[:tokens, span] * first - scores[tokens:, span] * second).astype(
                jnp.bfloat16
            )
            summed = summed + jnp.dot(
                weights, keyval[span, value_lo : value_lo + 128], preferred_element_type=jnp.float32
            )
        return summed

    def normed(summed, gain):
        power = jnp.mean(summed * summed, axis=-1, keepdims=True)
        return (summed * lax.rsqrt(power + EPSILON) * gain[...] * HEAD_SCALE).astype(jnp.bfloat16)

    for number in range(slots):
        summed = group(number, 0, DK_A, 0, 256, balance_a[z])
        out[z ^ number, :, 0:128] = normed(summed, gain_a)
        summed = group(number, 128, DK_B, 128, 128, balance_b[z])[:, 64:128]
        out[z ^ number, :, 128:192] = normed(summed, gain_b)


def project_kernel(slots, half, index, *refs):
    pieces, out_a, out_b, own, other, left = (
        refs[:slots],
        refs[slots],
        refs[slots + 1],
        refs[slots + 2],
        refs[slots + 3],
        refs[slots + 4],
    )
    z, core = index[0], index[2]
    mine = pl.multiple_of(core * half, half)
    theirs = pl.multiple_of((1 - core) * half, half)
    for k in range(slots):
        left[k, :half] = pieces[k][pl.ds(mine, half), :]
        left[k, half:] = pieces[k][pl.ds(theirs, half), :]
    tile = 512
    for n in range(out_a.shape[1] // tile):
        span = slice(n * tile, (n + 1) * tile)
        total = jnp.zeros((2 * half, tile), jnp.float32)
        for k in range(slots):
            head = z ^ k
            total += jnp.dot(
                left[k, :, 0:128],
                out_a[pl.ds(pl.multiple_of(head * 128, 128), 128), span],
                preferred_element_type=jnp.float32,
            )
            total += jnp.dot(
                left[k, :, 128:192],
                out_b[pl.ds(pl.multiple_of(head * 64, 64), 64), span],
                preferred_element_type=jnp.float32,
            )
        total = total.astype(jnp.bfloat16)
        own[:, span] = total[:half]
        other[:, span] = total[half:]


def norm_kernel(half, index, residual, own, other, gain, mixed, normed):
    mine = pl.multiple_of(index[2] * half, half)
    total = own[...].astype(jnp.float32) + other[...].astype(jnp.float32)
    rounded = (residual[pl.ds(mine, half), :].astype(jnp.float32) + total).astype(jnp.bfloat16)
    mixed[...] = rounded
    value = rounded.astype(jnp.float32)
    power = jnp.mean(value * value, axis=-1, keepdims=True)
    normed[...] = (value * lax.rsqrt(power + EPSILON) * gain[...]).astype(jnp.bfloat16)


def mixer_kernel(slots, plane, index, *refs):
    rows, refs = refs[: 2 * slots], refs[2 * slots :]
    ups, downs = refs[:plane], refs[plane : 2 * plane]
    own, other, left, hidden = refs[2 * plane :]
    z, g = index[0], index[1]
    half = rows[0].shape[0]
    block = ups[0].shape[0] // slots
    width = ups[0].shape[1]
    every = 2 * slots * half

    def place(k, p):
        return pl.ds(pl.multiple_of(((z ^ k) * plane + (g ^ p)) * block, block), block)

    for r, piece in enumerate(rows):
        for p in range(plane):
            for k in range(slots):
                at = (p * slots + k) * block
                left[r * half : (r + 1) * half, at : at + block] = piece[:, place(k, p)]
    tile = 256
    for n in range(width // tile):
        span = slice(n * tile, (n + 1) * tile)
        total = jnp.zeros((every, tile), jnp.float32)
        for p in range(plane):
            part = slots * block
            total += jnp.dot(
                left[:, p * part : (p + 1) * part],
                ups[p][:, span],
                preferred_element_type=jnp.float32,
            )
        active = jnp.maximum(total, 0.0)
        hidden[:, span] = (active * active).astype(jnp.bfloat16)
    for p in range(plane):
        for pair in range(0, slots, 2):
            part = lax.dot_general(
                hidden[...],
                downs[p][pair * block : (pair + 2) * block, :],
                (((1,), (1,)), ((), ())),
                preferred_element_type=jnp.float32,
            ).astype(jnp.bfloat16)
            for k in (pair, pair + 1):
                at = (k - pair) * block
                for r in range(slots):
                    rest = (r + slots) * half
                    own[r, :, place(k, p)] = part[r * half : (r + 1) * half, at : at + block]
                    other[r, :, place(k, p)] = part[rest : rest + half, at : at + block]


def fast_body(slots, plane, *arguments):
    (
        residual,
        query_first,
        key_first,
        value_first,
        query_second,
        key_second,
        value_second,
        balance_first,
        balance_second,
        head_gain_first,
        head_gain_second,
        out_first,
        out_second,
        mlp_gain,
        up_weight,
        down_weight,
    ) = arguments
    count = slots * plane
    tokens, width = residual.shape
    half = tokens // 2
    device, core = lax.axis_index("sp"), lax.axis_index("tp")
    z, g = device // plane, device % plane
    index = jnp.stack([z, g, core]).astype(jnp.int32)

    def along(value, k):
        if k == 0:
            return value
        return lax.ppermute(
            value, "sp", [(i, (i // plane ^ k) * plane + i % plane) for i in range(count)]
        )

    def across(value, k):
        if k == 0:
            return value
        return lax.ppermute(value, "sp", [(i, i ^ k) for i in range(count)])

    def swap(value):
        return lax.ppermute(value, "tp", [(0, 1), (1, 0)])

    packed = jnp.concatenate(
        [key_first, key_second, value_second, value_first, query_first, query_second], axis=2
    ).transpose(1, 0, 2)
    got = [along(lax.dynamic_index_in_dim(packed, z ^ k, 0, False), k) for k in range(slots)]
    keyval = jnp.stack([piece[:, :384] for piece in got])
    queries = [piece[:, 384:] for piece in got]
    kv_pieces = [across(keyval, p) for p in range(plane)]

    up_weight, down_weight, keyval = lax.optimization_barrier((up_weight, down_weight, keyval))
    hidden = up_weight.shape[1] // slots

    def spread(weight):
        parts = [
            along(lax.dynamic_slice_in_dim(weight, (z ^ k) * hidden, hidden, 1), k)
            for k in range(slots)
        ]
        mine = jnp.concatenate(parts, axis=0)
        return [across(mine, p) for p in range(plane)]

    ups = spread(up_weight)
    downs = spread(down_weight)

    smem = pl.BlockSpec(memory_space=SMEM)
    sequence = count * tokens
    heads = pl.pallas_call(
        functools.partial(attend_kernel, slots, plane, tokens),
        out_shape=jax.ShapeDtypeStruct((slots, tokens, 192), jnp.bfloat16),
        in_specs=[smem] * 3 + vmem_specs(2 + slots + plane),
        out_specs=pl.BlockSpec(memory_space=VMEM),
        scratch_shapes=[
            VMEM((slots, tokens, 192), jnp.bfloat16),
            VMEM((sequence, 384), jnp.bfloat16),
            VMEM((2 * tokens, sequence), jnp.float32),
        ],
        cost_estimate=pl.CostEstimate(flops=8 * 10**9, bytes_accessed=2 * 10**6, transcendentals=0),
        name="attend",
    )(
        index,
        balance_first,
        balance_second,
        head_gain_first[None],
        head_gain_second[None],
        *queries,
        *kv_pieces,
    )
    pieces = [along(heads[k], k) for k in range(slots)]
    row_shape = jax.ShapeDtypeStruct((half, width), jnp.bfloat16)
    own, other = pl.pallas_call(
        functools.partial(project_kernel, slots, half),
        out_shape=(row_shape, row_shape),
        in_specs=[smem] + vmem_specs(slots + 2),
        out_specs=tuple(vmem_specs(2)),
        scratch_shapes=[VMEM((slots, tokens, 192), jnp.bfloat16)],
        cost_estimate=pl.CostEstimate(flops=2 * 10**9, bytes_accessed=4 * 10**6, transcendentals=0),
        name="project",
    )(index, *pieces, out_first, out_second)
    mixed, normed = pl.pallas_call(
        functools.partial(norm_kernel, half),
        out_shape=(row_shape, row_shape),
        in_specs=[smem] + vmem_specs(4),
        out_specs=tuple(vmem_specs(2)),
        cost_estimate=pl.CostEstimate(flops=10**9, bytes_accessed=10**6, transcendentals=0),
        name="norm",
    )(index, residual, own, swap(other), mlp_gain[None])
    own_rows = [along(normed, k) for k in range(slots)]
    other_rows = [swap(piece) for piece in own_rows]
    part_shape = jax.ShapeDtypeStruct((slots, half, width), jnp.bfloat16)
    own, other = pl.pallas_call(
        functools.partial(mixer_kernel, slots, plane),
        out_shape=(part_shape, part_shape),
        in_specs=[smem] + vmem_specs(2 * slots + 2 * plane),
        out_specs=tuple(vmem_specs(2)),
        scratch_shapes=[
            VMEM((2 * slots * half, width), jnp.bfloat16),
            VMEM((2 * slots * half, hidden), jnp.bfloat16),
        ],
        cost_estimate=pl.CostEstimate(flops=6 * 10**9, bytes_accessed=10**7, transcendentals=0),
        name="mixer",
    )(index, *own_rows, *other_rows, *ups, *downs)
    summed = own.astype(jnp.float32) + swap(other).astype(jnp.float32)
    sent = summed.astype(jnp.bfloat16)
    total = summed[0]
    for k in range(1, slots):
        total = total + along(sent[k], k).astype(jnp.float32)
    mine = (mixed.astype(jnp.float32) + total).astype(jnp.bfloat16)
    theirs = swap(mine)
    return jnp.where(
        core == 0, jnp.concatenate([mine, theirs]), jnp.concatenate([theirs, mine])
    )


def dispatch(count, cores, *arguments):
    heads, other_heads = arguments[1].shape[1], arguments[4].shape[1]
    plane = count // heads
    fits = (
        cores == 2
        and heads == other_heads
        and plane == 4
        and plane * heads == count
        and arguments[3].shape[2] == 128
        and arguments[6].shape[2] == 64
    )
    if fits:
        return fast_body(heads, plane, *arguments)
    return body(*arguments)


def plan(mesh):
    return functools.partial(dispatch, mesh.shape["sp"], mesh.shape["tp"])


def solution(mesh):
    in_specs = (
        P("sp", None),
        P("sp", "tp", None),
        P("sp", "tp", None),
        P("sp", "tp", None),
        P("sp", "tp", None),
        P("sp", "tp", None),
        P("sp", "tp", None),
        P("tp"),
        P("tp"),
        P(),
        P(),
        P("tp", None),
        P("tp", None),
        P(),
        P("sp", "tp"),
        P("sp", "tp"),
    )
    out_specs = P("sp", None)
    chosen = plan(mesh)
    return jax.shard_map(chosen, mesh=mesh, in_specs=in_specs, out_specs=out_specs, check_vma=False)
```

```python
import functools
import math

import jax
import jax.numpy as jnp
from jax import lax
from jax.experimental import pallas as pl
from jax.experimental.pallas import tpu as pltpu
from jax.sharding import PartitionSpec as P

DK_A = 64
DK_B = 32


EPSILON = 1e-06
HEAD_SCALE = 0.8


def attend(queries, keys, values, balance, gain, device, head_size):
    tokens = queries.shape[0]
    heads = queries.shape[1]
    seq = keys.shape[0]
    depth = values.shape[2]
    block = math.gcd(512, seq)
    scale = head_size ** (-0.5)
    query_maps = queries.reshape(tokens, heads, 2, head_size)
    key_maps = keys.reshape(seq, heads, 2, head_size)
    first_row = device * tokens
    positions = first_row + jnp.arange(tokens, dtype=jnp.int32)
    needed = (first_row + tokens + block - 1) // block

    def block_scores(number):
        start = number * block
        key_block = lax.dynamic_slice_in_dim(key_maps, start, block, 0)
        scores = (
            jnp.einsum("qhmd,khmd->hmqk", query_maps, key_block, preferred_element_type=jnp.float32)
            * scale
        )
        columns = start + jnp.arange(block, dtype=jnp.int32)
        visible = columns[None, :] <= positions[:, None]
        return (jnp.where(visible, scores, -jnp.inf), start)

    def statistics(number, carry):
        highest, total = carry
        scores, _ = block_scores(number)
        fresh = jnp.maximum(highest, jnp.max(scores, axis=-1, keepdims=True))
        total = total * jnp.exp(highest - fresh) + jnp.sum(
            jnp.exp(scores - fresh), axis=-1, keepdims=True
        )
        return (fresh, total)

    start_high = jnp.full((heads, 2, tokens, 1), -jnp.inf, jnp.float32)
    start_total = jnp.zeros((heads, 2, tokens, 1), jnp.float32)
    highest, total = lax.fori_loop(0, needed, statistics, (start_high, start_total))

    def accumulate(number, result):
        scores, start = block_scores(number)
        probs = jnp.exp(scores - highest) / total
        mixed = (probs[:, 0] - balance[:, None, None] * probs[:, 1]).astype(jnp.bfloat16)
        value_block = lax.dynamic_slice_in_dim(values, start, block, 0)
        return result + jnp.einsum(
            "hqk,khe->qhe", mixed, value_block, preferred_element_type=jnp.float32
        )

    summed = lax.fori_loop(0, needed, accumulate, jnp.zeros((tokens, heads, depth), jnp.float32))
    power = jnp.mean(summed * summed, axis=-1, keepdims=True)
    normed = summed * lax.rsqrt(power + EPSILON) * gain * HEAD_SCALE
    return normed.astype(jnp.bfloat16).reshape(tokens, heads * depth)


def body(
    residual,
    query_first,
    key_first,
    value_first,
    query_second,
    key_second,
    value_second,
    balance_first,
    balance_second,
    head_gain_first,
    head_gain_second,
    out_first,
    out_second,
    mlp_gain,
    up_weight,
    down_weight,
):
    device = lax.axis_index("sp")
    keys_first, values_first, keys_second, values_second = (
        lax.all_gather(key_first, "sp", axis=0, tiled=True),
        lax.all_gather(value_first, "sp", axis=0, tiled=True),
        lax.all_gather(key_second, "sp", axis=0, tiled=True),
        lax.all_gather(value_second, "sp", axis=0, tiled=True),
    )
    heads_first = attend(
        query_first, keys_first, values_first, balance_first, head_gain_first, device, DK_A
    )
    heads_second = attend(
        query_second, keys_second, values_second, balance_second, head_gain_second, device, DK_B
    )
    head_term = jnp.dot(heads_first, out_first, preferred_element_type=jnp.float32) + jnp.dot(
        heads_second, out_second, preferred_element_type=jnp.float32
    )
    head_total = lax.psum(head_term.astype(jnp.bfloat16), "tp").astype(jnp.float32)
    mixed = (residual.astype(jnp.float32) + head_total).astype(jnp.bfloat16)
    mixed_float = mixed.astype(jnp.float32)
    power = jnp.mean(mixed_float * mixed_float, axis=-1, keepdims=True)
    normed = (mixed_float * lax.rsqrt(power + EPSILON) * mlp_gain).astype(jnp.bfloat16)
    up_whole, down_whole = (
        lax.all_gather(up_weight, "sp", axis=0, tiled=True),
        lax.all_gather(down_weight, "sp", axis=0, tiled=True),
    )
    lifted = jnp.dot(normed, up_whole, preferred_element_type=jnp.float32)
    active = jax.nn.relu(lifted)
    hidden = (active * active).astype(jnp.bfloat16)
    down_term = lax.dot_general(
        hidden, down_whole, (((1,), (1,)), ((), ())), preferred_element_type=jnp.float32
    )
    added = lax.psum(down_term.astype(jnp.bfloat16), "tp").astype(jnp.float32)
    return (mixed_float + added).astype(jnp.bfloat16)


VMEM = pltpu.VMEM
SMEM = pltpu.SMEM


def vmem_specs(count):
    return [pl.BlockSpec(memory_space=VMEM)] * count


def pack_kernel(slots, index, key_a, key_b, value_b, value_a, query_a, query_b, *refs):
    outs, packed = refs[:slots], refs[slots]
    for head in range(slots):
        packed[head, :, 0:128] = key_a[:, head, :]
        packed[head, :, 128:192] = key_b[head].T
        packed[head, :, 192:256] = value_b[head].T
        packed[head, :, 256:384] = value_a[:, head, :]
        packed[head, :, 384:512] = query_a[:, head, :]
        packed[head, :, 512:576] = query_b[head].T
    for k in range(slots):
        outs[k][...] = packed[index[0] ^ k]


def attend_kernel(slots, plane, tokens, index, balance_a, balance_b, gain_a, gain_b, *refs):
    queries, kv_pieces = refs[:slots], refs[slots : slots + plane]
    outs = refs[slots + plane : 2 * slots + plane]
    query, keyval, scores, out = refs[2 * slots + plane :]
    z, g = index[0], index[1]
    wide = plane * tokens
    for k in range(slots):
        query[z ^ k] = queries[k][:, 384:576]
        for p in range(plane):
            start = pl.multiple_of(((z ^ k) * plane + (g ^ p)) * tokens, tokens)
            keyval[pl.ds(start, tokens), :] = kv_pieces[p][k]
    lane = lax.broadcasted_iota(jnp.int32, (tokens, 128), 1)
    row = lax.broadcasted_iota(jnp.int32, (2 * tokens, wide), 0) % tokens
    column = lax.broadcasted_iota(jnp.int32, (2 * tokens, wide), 1)
    visible = column <= row + g * tokens

    def group(number, place, size, key_lo, value_lo, balance):
        packed = query[number][:, place : place + 2 * size]
        if 2 * size < 128:
            packed = jnp.concatenate(
                [packed, jnp.zeros((tokens, 128 - 2 * size), packed.dtype)], axis=1
            )
        zero = jnp.zeros_like(packed)
        both = jnp.concatenate(
            [jnp.where(lane < size, packed, zero), jnp.where(lane >= size, packed, zero)], axis=0
        )
        factor = size ** (-0.5) * math.log2(math.e)
        highest = None
        for c in range(number + 1):
            part = lax.dot_general(
                both,
                keyval[c * wide : (c + 1) * wide, key_lo : key_lo + 128],
                (((1,), (1,)), ((), ())),
                preferred_element_type=jnp.float32,
            )
            if c == number:
                part = jnp.where(visible, part, -jnp.inf)
            scores[:, c * wide : (c + 1) * wide] = part
            top = jnp.max(part, axis=1, keepdims=True)
            highest = top if highest is None else jnp.maximum(highest, top)
        total = jnp.zeros((2 * tokens, 1), jnp.float32)
        for c in range(number + 1):
            part = jnp.exp2((scores[:, c * wide : (c + 1) * wide] - highest) * factor)
            scores[:, c * wide : (c + 1) * wide] = part
            total = total + jnp.sum(part, axis=1, keepdims=True)
        share = 1.0 / total
        first, second = share[:tokens], share[tokens:] * balance
        summed = jnp.zeros((tokens, 128), jnp.float32)
        for c in range(number + 1):
            span = slice(c * wide, (c + 1) * wide)
            weights = (scores[:tokens, span] * first - scores[tokens:, span] * second).astype(
                jnp.bfloat16
            )
            summed = summed + jnp.dot(
                weights, keyval[span, value_lo : value_lo + 128], preferred_element_type=jnp.float32
            )
        return summed

    def normed(summed, gain):
        power = jnp.mean(summed * summed, axis=-1, keepdims=True)
        return (summed * lax.rsqrt(power + EPSILON) * gain[...] * HEAD_SCALE).astype(jnp.bfloat16)

    for number in range(slots):
        summed = group(number, 0, DK_A, 0, 256, balance_a[z])
        out[number, :, 0:128] = normed(summed, gain_a)
        summed = group(number, 128, DK_B, 128, 128, balance_b[z])[:, 64:128]
        out[number, :, 128:192] = normed(summed, gain_b)
    for k in range(slots):
        outs[k][...] = out[z ^ k]


def project_kernel(slots, half, index, *refs):
    pieces, out_a, out_b, own, other, left = (
        refs[:slots],
        refs[slots],
        refs[slots + 1],
        refs[slots + 2],
        refs[slots + 3],
        refs[slots + 4],
    )
    z, core = index[0], index[2]
    mine = pl.multiple_of(core * half, half)
    theirs = pl.multiple_of((1 - core) * half, half)
    for k in range(slots):
        left[k, :half] = pieces[k][pl.ds(mine, half), :]
        left[k, half:] = pieces[k][pl.ds(theirs, half), :]
    tile = 512
    for n in range(out_a.shape[1] // tile):
        span = slice(n * tile, (n + 1) * tile)
        total = jnp.zeros((2 * half, tile), jnp.float32)
        for k in range(slots):
            head = z ^ k
            total += jnp.dot(
                left[k, :, 0:128],
                out_a[pl.ds(pl.multiple_of(head * 128, 128), 128), span],
                preferred_element_type=jnp.float32,
            )
            total += jnp.dot(
                left[k, :, 128:192],
                out_b[pl.ds(pl.multiple_of(head * 64, 64), 64), span],
                preferred_element_type=jnp.float32,
            )
        total = total.astype(jnp.bfloat16)
        own[:, span] = total[:half]
        other[:, span] = total[half:]


def norm_kernel(half, index, residual, own, other, gain, mixed, normed):
    mine = pl.multiple_of(index[2] * half, half)
    total = own[...].astype(jnp.float32) + other[...].astype(jnp.float32)
    rounded = (residual[pl.ds(mine, half), :].astype(jnp.float32) + total).astype(jnp.bfloat16)
    mixed[...] = rounded
    value = rounded.astype(jnp.float32)
    power = jnp.mean(value * value, axis=-1, keepdims=True)
    normed[...] = (value * lax.rsqrt(power + EPSILON) * gain[...]).astype(jnp.bfloat16)


def arrange_kernel(slots, plane, first, split, index, *refs):
    firsts, rests, far, out = refs[:plane], refs[plane : 2 * plane - 1], refs[-3:-1], refs[-1]
    z, g = index[0], index[1]
    block = out.shape[0] // (slots * plane)

    def put(k, p, value):
        place = pl.multiple_of(((z ^ k) * plane + (g ^ p)) * block, block)
        out[pl.ds(place, block), :] = value

    for p in range(plane):
        put(0, p, firsts[p][first * block : (first + 1) * block, :])
        for k in range(1, slots):
            if p < plane - 1:
                put(k, p, rests[p][(k - 1) * block : k * block, :])
            elif k <= split:
                put(k, p, far[0][(k - 1) * block : k * block, :])
            else:
                put(k, p, far[1][(k - 1 - split) * block : (k - split) * block, :])


def lift_kernel(up, *refs):
    rows, hidden, left = refs[:-2], refs[-2], refs[-1]
    half = rows[0].shape[0]
    for r, piece in enumerate(rows):
        left[r * half : (r + 1) * half, :] = piece[...]
    tile = 256
    for n in range(up.shape[1] // tile):
        span = slice(n * tile, (n + 1) * tile)
        active = jnp.maximum(
            jnp.dot(left[...], up[:, span], preferred_element_type=jnp.float32), 0.0
        )
        hidden[:, span] = (active * active).astype(jnp.bfloat16)


def lower_kernel(hidden, down, own, other):
    count, half, width = own.shape
    tile = 512
    for n in range(width // tile):
        span = slice(n * tile, (n + 1) * tile)
        part = lax.dot_general(
            hidden[...],
            down[span, :],
            (((1,), (1,)), ((), ())),
            preferred_element_type=jnp.float32,
        ).astype(jnp.bfloat16)
        for r in range(count):
            rest = (r + count) * half
            own[r, :, span] = part[r * half : (r + 1) * half]
            other[r, :, span] = part[rest : rest + half]


def fast_body(slots, plane, *arguments):
    (
        residual,
        query_first,
        key_first,
        value_first,
        query_second,
        key_second,
        value_second,
        balance_first,
        balance_second,
        head_gain_first,
        head_gain_second,
        out_first,
        out_second,
        mlp_gain,
        up_weight,
        down_weight,
    ) = arguments
    count = slots * plane
    tokens, width = residual.shape
    half = tokens // 2
    device, core = lax.axis_index("sp"), lax.axis_index("tp")
    z, g = device // plane, device % plane
    index = jnp.stack([z, g, core]).astype(jnp.int32)

    def along(value, k):
        if k == 0:
            return value
        return lax.ppermute(
            value, "sp", [(i, (i // plane ^ k) * plane + i % plane) for i in range(count)]
        )

    def across(value, k):
        if k == 0:
            return value
        return lax.ppermute(value, "sp", [(i, i ^ k) for i in range(count)])

    def swap(value):
        return lax.ppermute(value, "tp", [(0, 1), (1, 0)])

    smem = pl.BlockSpec(memory_space=SMEM)
    packed = pl.pallas_call(
        functools.partial(pack_kernel, slots),
        out_shape=(jax.ShapeDtypeStruct((tokens, 576), jnp.bfloat16),) * slots,
        in_specs=[smem] + vmem_specs(6),
        out_specs=tuple(vmem_specs(slots)),
        scratch_shapes=[VMEM((slots, tokens, 576), jnp.bfloat16)],
        compiler_params=pltpu.CompilerParams(vmem_limit_bytes=8 * 2**20),
                cost_estimate=pl.CostEstimate(flops=10**8, bytes_accessed=10**6, transcendentals=0),
        name="pack",
    )(
        index,
        key_first,
        key_second.transpose(1, 2, 0),
        value_second.transpose(1, 2, 0),
        value_first,
        query_first,
        query_second.transpose(1, 2, 0),
    )
    got = [along(packed[k], k) for k in range(slots)]
    keyval = jnp.stack([piece[:, :384] for piece in got])
    kv_pieces = [across(keyval, p) for p in range(plane)]

    hidden = up_weight.shape[1] // slots

    def column(weight, k):
        return lax.dynamic_slice_in_dim(weight, (z ^ k) * hidden, hidden, 1)

    early = jnp.concatenate([column(up_weight, 0), column(down_weight, 0)], axis=0)
    firsts = [across(early, p) for p in range(plane)]
    block = up_weight.shape[0]

    def spread(weight, first, split):
        parts = [along(column(weight, k), k) for k in range(1, slots)]
        mine = jnp.concatenate(parts, axis=0)
        near = [across(mine, p) for p in (1, 2)]
        way = 1 if first == 0 else 2
        far = [
            across(near[2 - way][: split * block], way),
            across(near[way - 1][split * block :], 3 - way),
        ]
        return pl.pallas_call(
            functools.partial(arrange_kernel, slots, plane, first, split),
            out_shape=jax.ShapeDtypeStruct((count * block, hidden), jnp.bfloat16),
            in_specs=[smem] + vmem_specs(2 * plane + 1),
            out_specs=pl.BlockSpec(memory_space=VMEM),
            compiler_params=pltpu.CompilerParams(vmem_limit_bytes=16 * 2**20),
            cost_estimate=pl.CostEstimate(flops=10**8, bytes_accessed=10**6, transcendentals=0),
        )(index, *firsts, mine, *near, *far)

    up = spread(up_weight, 0, 2)
    down = spread(down_weight, 1, 2)

    sequence = count * tokens
    heads = pl.pallas_call(
        functools.partial(attend_kernel, slots, plane, tokens),
        out_shape=(jax.ShapeDtypeStruct((tokens, 192), jnp.bfloat16),) * slots,
        in_specs=[smem] * 3 + vmem_specs(2 + slots + plane),
        out_specs=tuple(vmem_specs(slots)),
        compiler_params=pltpu.CompilerParams(vmem_limit_bytes=24 * 2**20),
                scratch_shapes=[
            VMEM((slots, tokens, 192), jnp.bfloat16),
            VMEM((sequence, 384), jnp.bfloat16),
            VMEM((2 * tokens, sequence), jnp.float32),
            VMEM((slots, tokens, 192), jnp.bfloat16),
        ],
        cost_estimate=pl.CostEstimate(flops=8 * 10**9, bytes_accessed=2 * 10**6, transcendentals=0),
        name="attend",
    )(
        index,
        balance_first,
        balance_second,
        head_gain_first[None],
        head_gain_second[None],
        *got,
        *kv_pieces,
    )
    pieces = [along(heads[k], k) for k in range(slots)]
    row_shape = jax.ShapeDtypeStruct((half, width), jnp.bfloat16)
    own, other = pl.pallas_call(
        functools.partial(project_kernel, slots, half),
        out_shape=(row_shape, row_shape),
        in_specs=[smem] + vmem_specs(slots + 2),
        out_specs=tuple(vmem_specs(2)),
        scratch_shapes=[VMEM((slots, tokens, 192), jnp.bfloat16)],
        compiler_params=pltpu.CompilerParams(vmem_limit_bytes=16 * 2**20),
                cost_estimate=pl.CostEstimate(flops=2 * 10**9, bytes_accessed=4 * 10**6, transcendentals=0),
        name="project",
    )(index, *pieces, out_first, out_second)
    mixed, normed = pl.pallas_call(
        functools.partial(norm_kernel, half),
        out_shape=(row_shape, row_shape),
        in_specs=[smem] + vmem_specs(4),
        out_specs=tuple(vmem_specs(2)),
        compiler_params=pltpu.CompilerParams(vmem_limit_bytes=8 * 2**20),
                cost_estimate=pl.CostEstimate(flops=10**9, bytes_accessed=10**6, transcendentals=0),
        name="norm",
    )(index, residual, own, swap(other), mlp_gain[None])
    own_rows = [along(normed, k) for k in range(slots)]
    other_rows = [swap(piece) for piece in own_rows]
    group = slots // 2
    part_shape = jax.ShapeDtypeStruct((group, half, width), jnp.bfloat16)
    total = None

    def lift(lo):
        chosen = own_rows[lo : lo + group] + other_rows[lo : lo + group]
        return pl.pallas_call(
            lift_kernel,
            out_shape=jax.ShapeDtypeStruct((2 * group * half, hidden), jnp.bfloat16),
            in_specs=vmem_specs(1 + 2 * group),
            out_specs=pl.BlockSpec(memory_space=VMEM),
            scratch_shapes=[VMEM((2 * group * half, width), jnp.bfloat16)],
            compiler_params=pltpu.CompilerParams(vmem_limit_bytes=16 * 2**20),
            cost_estimate=pl.CostEstimate(flops=3 * 10**9, bytes_accessed=10**6, transcendentals=0),
        )(up, *chosen)

    def lower(active):
        return pl.pallas_call(
            lower_kernel,
            out_shape=(part_shape, part_shape),
            in_specs=vmem_specs(2),
            out_specs=tuple(vmem_specs(2)),
            compiler_params=pltpu.CompilerParams(vmem_limit_bytes=16 * 2**20),
            cost_estimate=pl.CostEstimate(flops=3 * 10**9, bytes_accessed=10**6, transcendentals=0),
        )(active, down)

    actives = {lo: lift(lo) for lo in (0, group)}
    terms = {}
    for lo in (group, 0):
        own, other = lower(actives[lo])
        summed = own.astype(jnp.float32) + swap(other).astype(jnp.float32)
        for k in range(lo, lo + group):
            piece = summed[k - lo]
            terms[k] = piece if k == 0 else along(piece.astype(jnp.bfloat16), k)
    total = terms[0]
    for k in range(1, slots):
        total = total + terms[k].astype(jnp.float32)
    mine = (mixed.astype(jnp.float32) + total).astype(jnp.bfloat16)
    theirs = swap(mine)
    return jnp.where(
        core == 0, jnp.concatenate([mine, theirs]), jnp.concatenate([theirs, mine])
    )


def dispatch(count, cores, *arguments):
    heads, other_heads = arguments[1].shape[1], arguments[4].shape[1]
    plane = count // heads
    fits = (
        cores == 2
        and heads == other_heads
        and plane == 4
        and plane * heads == count
        and arguments[3].shape[2] == 128
        and arguments[6].shape[2] == 64
    )
    if fits:
        return fast_body(heads, plane, *arguments)
    return body(*arguments)


def plan(mesh):
    return functools.partial(dispatch, mesh.shape["sp"], mesh.shape["tp"])


def solution(mesh):
    in_specs = (
        P("sp", None),
        P("sp", "tp", None),
        P("sp", "tp", None),
        P("sp", "tp", None),
        P("sp", "tp", None),
        P("sp", "tp", None),
        P("sp", "tp", None),
        P("tp"),
        P("tp"),
        P(),
        P(),
        P("tp", None),
        P("tp", None),
        P(),
        P("sp", "tp"),
        P("sp", "tp"),
    )
    out_specs = P("sp", None)
    return jax.shard_map(
        plan(mesh), mesh=mesh, in_specs=in_specs, out_specs=out_specs, check_vma=False
    )
```

```python
import functools
import math

import jax
import jax.numpy as jnp
from jax import lax
from jax.experimental import pallas as pl
from jax.experimental.pallas import tpu as pltpu
from jax.sharding import PartitionSpec as P

DK_A = 64
DK_B = 32


EPSILON = 1e-06
HEAD_SCALE = 0.8


def attend(queries, keys, values, balance, gain, device, head_size):
    tokens = queries.shape[0]
    heads = queries.shape[1]
    seq = keys.shape[0]
    depth = values.shape[2]
    block = math.gcd(512, seq)
    scale = head_size ** (-0.5)
    query_maps = queries.reshape(tokens, heads, 2, head_size)
    key_maps = keys.reshape(seq, heads, 2, head_size)
    first_row = device * tokens
    positions = first_row + jnp.arange(tokens, dtype=jnp.int32)
    needed = (first_row + tokens + block - 1) // block

    def block_scores(number):
        start = number * block
        key_block = lax.dynamic_slice_in_dim(key_maps, start, block, 0)
        scores = (
            jnp.einsum("qhmd,khmd->hmqk", query_maps, key_block, preferred_element_type=jnp.float32)
            * scale
        )
        columns = start + jnp.arange(block, dtype=jnp.int32)
        visible = columns[None, :] <= positions[:, None]
        return (jnp.where(visible, scores, -jnp.inf), start)

    def statistics(number, carry):
        highest, total = carry
        scores, _ = block_scores(number)
        fresh = jnp.maximum(highest, jnp.max(scores, axis=-1, keepdims=True))
        total = total * jnp.exp(highest - fresh) + jnp.sum(
            jnp.exp(scores - fresh), axis=-1, keepdims=True
        )
        return (fresh, total)

    start_high = jnp.full((heads, 2, tokens, 1), -jnp.inf, jnp.float32)
    start_total = jnp.zeros((heads, 2, tokens, 1), jnp.float32)
    highest, total = lax.fori_loop(0, needed, statistics, (start_high, start_total))

    def accumulate(number, result):
        scores, start = block_scores(number)
        probs = jnp.exp(scores - highest) / total
        mixed = (probs[:, 0] - balance[:, None, None] * probs[:, 1]).astype(jnp.bfloat16)
        value_block = lax.dynamic_slice_in_dim(values, start, block, 0)
        return result + jnp.einsum(
            "hqk,khe->qhe", mixed, value_block, preferred_element_type=jnp.float32
        )

    summed = lax.fori_loop(0, needed, accumulate, jnp.zeros((tokens, heads, depth), jnp.float32))
    power = jnp.mean(summed * summed, axis=-1, keepdims=True)
    normed = summed * lax.rsqrt(power + EPSILON) * gain * HEAD_SCALE
    return normed.astype(jnp.bfloat16).reshape(tokens, heads * depth)


def body(
    residual,
    query_first,
    key_first,
    value_first,
    query_second,
    key_second,
    value_second,
    balance_first,
    balance_second,
    head_gain_first,
    head_gain_second,
    out_first,
    out_second,
    mlp_gain,
    up_weight,
    down_weight,
):
    device = lax.axis_index("sp")
    keys_first, values_first, keys_second, values_second = (
        lax.all_gather(key_first, "sp", axis=0, tiled=True),
        lax.all_gather(value_first, "sp", axis=0, tiled=True),
        lax.all_gather(key_second, "sp", axis=0, tiled=True),
        lax.all_gather(value_second, "sp", axis=0, tiled=True),
    )
    heads_first = attend(
        query_first, keys_first, values_first, balance_first, head_gain_first, device, DK_A
    )
    heads_second = attend(
        query_second, keys_second, values_second, balance_second, head_gain_second, device, DK_B
    )
    head_term = jnp.dot(heads_first, out_first, preferred_element_type=jnp.float32) + jnp.dot(
        heads_second, out_second, preferred_element_type=jnp.float32
    )
    head_total = lax.psum(head_term.astype(jnp.bfloat16), "tp").astype(jnp.float32)
    mixed = (residual.astype(jnp.float32) + head_total).astype(jnp.bfloat16)
    mixed_float = mixed.astype(jnp.float32)
    power = jnp.mean(mixed_float * mixed_float, axis=-1, keepdims=True)
    normed = (mixed_float * lax.rsqrt(power + EPSILON) * mlp_gain).astype(jnp.bfloat16)
    up_whole, down_whole = (
        lax.all_gather(up_weight, "sp", axis=0, tiled=True),
        lax.all_gather(down_weight, "sp", axis=0, tiled=True),
    )
    lifted = jnp.dot(normed, up_whole, preferred_element_type=jnp.float32)
    active = jax.nn.relu(lifted)
    hidden = (active * active).astype(jnp.bfloat16)
    down_term = lax.dot_general(
        hidden, down_whole, (((1,), (1,)), ((), ())), preferred_element_type=jnp.float32
    )
    added = lax.psum(down_term.astype(jnp.bfloat16), "tp").astype(jnp.float32)
    return (mixed_float + added).astype(jnp.bfloat16)


VMEM = pltpu.VMEM
SMEM = pltpu.SMEM


def vmem_specs(count):
    return [pl.BlockSpec(memory_space=VMEM)] * count


def pack_kernel(slots, index, *refs):
    sources, outs, held = refs[:6], refs[6 : 6 + slots], refs[6 + slots : -2]
    packed, arrived = refs[-2:]
    copies = [
        pltpu.make_async_copy(source, target, arrived.at[i])
        for i, (source, target) in enumerate(zip(sources, held))
    ]
    for copy in copies:
        copy.start()
    for copy in copies:
        copy.wait()
    key_a, key_b, value_b, value_a, query_a, query_b = held
    for head in range(slots):
        packed[head, :, 0:128] = key_a[:, head, :]
        packed[head, :, 128:192] = key_b[head].T
        packed[head, :, 192:256] = value_b[head].T
        packed[head, :, 256:384] = value_a[:, head, :]
        packed[head, :, 384:512] = query_a[:, head, :]
        packed[head, :, 512:576] = query_b[head].T
    for k in range(slots):
        outs[k][...] = packed[index[0] ^ k]


def cut_kernel(slots, width, index, *refs):
    weights, pairs, ups, downs = refs[:2], refs[2:4], refs[4 : 2 + slots], refs[2 + slots : -1]
    arrived = refs[-1]
    block = weights[0].shape[0]
    copies = []
    for i, (weight, pieces) in enumerate(zip(weights, (ups, downs))):
        for k in range(slots):
            place = pl.ds(pl.multiple_of((index[0] ^ k) * width, width), width)
            target = pairs[k].at[pl.ds(i * block, block), :] if k < 2 else pieces[k - 2]
            copies.append(
                pltpu.make_async_copy(weight.at[:, place], target, arrived.at[i * slots + k])
            )
    for copy in copies:
        copy.start()
    for copy in copies:
        copy.wait()


def attend_kernel(slots, plane, tokens, index, balance_a, balance_b, gain_a, gain_b, *refs):
    queries, kv_pieces = refs[:slots], refs[slots : slots + plane + 1]
    outs = refs[slots + plane + 1 : 2 * slots + plane + 1]
    query, keyval, scores, out = refs[2 * slots + plane + 1 :]
    z, g = index[0], index[1]
    wide = plane * tokens
    for k in range(slots):
        query[z ^ k] = queries[k][:, 384:576]
        for p in range(plane):
            start = pl.multiple_of(((z ^ k) * plane + (g ^ p)) * tokens, tokens)
            if p < plane - 1:
                keyval[pl.ds(start, tokens), :] = kv_pieces[p][k]
            else:
                part = slots // 2
                keyval[pl.ds(start, tokens), :] = kv_pieces[p + k // part][k % part]
    lane = lax.broadcasted_iota(jnp.int32, (tokens, 128), 1)
    row = lax.broadcasted_iota(jnp.int32, (2 * tokens, wide), 0) % tokens
    column = lax.broadcasted_iota(jnp.int32, (2 * tokens, wide), 1)
    visible = column <= row + g * tokens

    def group(number, place, size, key_lo, value_lo, balance):
        packed = query[number][:, place : place + 2 * size]
        if 2 * size < 128:
            packed = jnp.concatenate(
                [packed, jnp.zeros((tokens, 128 - 2 * size), packed.dtype)], axis=1
            )
        zero = jnp.zeros_like(packed)
        both = jnp.concatenate(
            [jnp.where(lane < size, packed, zero), jnp.where(lane >= size, packed, zero)], axis=0
        )
        factor = size ** (-0.5) * math.log2(math.e)
        highest = None
        for c in range(number + 1):
            part = lax.dot_general(
                both,
                keyval[c * wide : (c + 1) * wide, key_lo : key_lo + 128],
                (((1,), (1,)), ((), ())),
                preferred_element_type=jnp.float32,
            )
            if c == number:
                part = jnp.where(visible, part, -jnp.inf)
            scores[:, c * wide : (c + 1) * wide] = part
            top = jnp.max(part, axis=1, keepdims=True)
            highest = top if highest is None else jnp.maximum(highest, top)
        total = jnp.zeros((2 * tokens, 1), jnp.float32)
        for c in range(number + 1):
            part = jnp.exp2((scores[:, c * wide : (c + 1) * wide] - highest) * factor)
            scores[:, c * wide : (c + 1) * wide] = part
            total = total + jnp.sum(part, axis=1, keepdims=True)
        share = 1.0 / total
        first, second = share[:tokens], share[tokens:] * balance
        summed = jnp.zeros((tokens, 128), jnp.float32)
        for c in range(number + 1):
            span = slice(c * wide, (c + 1) * wide)
            weights = (scores[:tokens, span] * first - scores[tokens:, span] * second).astype(
                jnp.bfloat16
            )
            summed = summed + jnp.dot(
                weights, keyval[span, value_lo : value_lo + 128], preferred_element_type=jnp.float32
            )
        return summed

    def normed(summed, gain):
        power = jnp.mean(summed * summed, axis=-1, keepdims=True)
        return (summed * lax.rsqrt(power + EPSILON) * gain[...] * HEAD_SCALE).astype(jnp.bfloat16)

    for number in range(slots):
        summed = group(number, 0, DK_A, 0, 256, balance_a[z])
        out[number, :, 0:128] = normed(summed, gain_a)
        summed = group(number, 128, DK_B, 128, 128, balance_b[z])[:, 64:128]
        out[number, :, 128:192] = normed(summed, gain_b)
    for k in range(slots):
        outs[k][...] = out[z ^ k]


def project_kernel(slots, half, index, *refs):
    pieces, out_a, out_b, own, other, left = (
        refs[:slots],
        refs[slots],
        refs[slots + 1],
        refs[slots + 2],
        refs[slots + 3],
        refs[slots + 4],
    )
    z, core = index[0], index[2]
    mine = pl.multiple_of(core * half, half)
    theirs = pl.multiple_of((1 - core) * half, half)
    for k in range(slots):
        left[k, :half] = pieces[k][pl.ds(mine, half), :]
        left[k, half:] = pieces[k][pl.ds(theirs, half), :]
    tile = 512
    for n in range(out_a.shape[1] // tile):
        span = slice(n * tile, (n + 1) * tile)
        total = jnp.zeros((2 * half, tile), jnp.float32)
        for k in range(slots):
            head = z ^ k
            total += jnp.dot(
                left[k, :, 0:128],
                out_a[pl.ds(pl.multiple_of(head * 128, 128), 128), span],
                preferred_element_type=jnp.float32,
            )
            total += jnp.dot(
                left[k, :, 128:192],
                out_b[pl.ds(pl.multiple_of(head * 64, 64), 64), span],
                preferred_element_type=jnp.float32,
            )
        total = total.astype(jnp.bfloat16)
        own[:, span] = total[:half]
        other[:, span] = total[half:]


def norm_kernel(half, index, residual, own, other, gain, mixed, normed):
    mine = pl.multiple_of(index[2] * half, half)
    total = own[...].astype(jnp.float32) + other[...].astype(jnp.float32)
    rounded = (residual[pl.ds(mine, half), :].astype(jnp.float32) + total).astype(jnp.bfloat16)
    mixed[...] = rounded
    value = rounded.astype(jnp.float32)
    power = jnp.mean(value * value, axis=-1, keepdims=True)
    normed[...] = (value * lax.rsqrt(power + EPSILON) * gain[...]).astype(jnp.bfloat16)


def arrange_kernel(moves, plane, block, index, *refs):
    out = refs[-1]
    z, g = index[0], index[1]
    for p, k, number, at in moves:
        place = pl.multiple_of(((z ^ k) * plane + (g ^ p)) * block, block)
        out[pl.ds(place, block), :] = refs[number][at * block : (at + 1) * block, :]


def lift_kernel(up, *refs):
    rows, hidden, left = refs[:-2], refs[-2], refs[-1]
    half = rows[0].shape[0]
    for r, piece in enumerate(rows):
        left[r * half : (r + 1) * half, :] = piece[...]
    tile = 256
    for n in range(up.shape[1] // tile):
        span = slice(n * tile, (n + 1) * tile)
        active = jnp.maximum(
            jnp.dot(left[...], up[:, span], preferred_element_type=jnp.float32), 0.0
        )
        hidden[:, span] = (active * active).astype(jnp.bfloat16)


def lower_kernel(hidden, down, own, other):
    count, half, width = own.shape
    tile = 512
    for n in range(width // tile):
        span = slice(n * tile, (n + 1) * tile)
        part = lax.dot_general(
            hidden[...],
            down[span, :],
            (((1,), (1,)), ((), ())),
            preferred_element_type=jnp.float32,
        ).astype(jnp.bfloat16)
        for r in range(count):
            rest = (r + count) * half
            own[r, :, span] = part[r * half : (r + 1) * half]
            other[r, :, span] = part[rest : rest + half]


def fast_body(slots, plane, *arguments):
    (
        residual,
        query_first,
        key_first,
        value_first,
        query_second,
        key_second,
        value_second,
        balance_first,
        balance_second,
        head_gain_first,
        head_gain_second,
        out_first,
        out_second,
        mlp_gain,
        up_weight,
        down_weight,
    ) = arguments
    count = slots * plane
    tokens, width = residual.shape
    half = tokens // 2
    device, core = lax.axis_index("sp"), lax.axis_index("tp")
    z, g = device // plane, device % plane
    index = jnp.stack([z, g, core]).astype(jnp.int32)

    def along(value, k):
        if k == 0:
            return value
        return lax.ppermute(
            value, "sp", [(i, (i // plane ^ k) * plane + i % plane) for i in range(count)]
        )

    def across(value, k):
        if k == 0:
            return value
        return lax.ppermute(value, "sp", [(i, i ^ k) for i in range(count)])

    def swap(value):
        return lax.ppermute(value, "tp", [(0, 1), (1, 0)])

    smem = pl.BlockSpec(memory_space=SMEM)
    hidden = up_weight.shape[1] // slots
    block = up_weight.shape[0]
    sources = (
        key_first,
        key_second.transpose(1, 2, 0),
        value_second.transpose(1, 2, 0),
        value_first,
        query_first,
        query_second.transpose(1, 2, 0),
    )
    packed = pl.pallas_call(
        functools.partial(pack_kernel, slots),
        out_shape=(jax.ShapeDtypeStruct((tokens, 576), jnp.bfloat16),) * slots,
        in_specs=[smem] + [pl.BlockSpec(memory_space=pltpu.HBM)] * 6,
        out_specs=tuple(vmem_specs(slots)),
        scratch_shapes=[VMEM(source.shape, jnp.bfloat16) for source in sources]
        + [VMEM((slots, tokens, 576), jnp.bfloat16), pltpu.SemaphoreType.DMA((6,))],
        cost_estimate=pl.CostEstimate(flops=10**8, bytes_accessed=10**6, transcendentals=0),
        name="pack",
    )(index, *sources)
    piece_shape = jax.ShapeDtypeStruct((block, hidden), jnp.bfloat16)
    cuts = pl.pallas_call(
        functools.partial(cut_kernel, slots, hidden),
        out_shape=(jax.ShapeDtypeStruct((2 * block, hidden), jnp.bfloat16),) * 2
        + (piece_shape,) * (2 * slots - 4),
        in_specs=[smem] + [pl.BlockSpec(memory_space=pltpu.HBM)] * 2,
        out_specs=tuple(vmem_specs(2 * slots - 2)),
        scratch_shapes=[pltpu.SemaphoreType.DMA((2 * slots,))],
        cost_estimate=pl.CostEstimate(flops=10**8, bytes_accessed=10**6, transcendentals=0),
        name="cut",
    )(index, up_weight, down_weight)
    early, both, cut_up, cut_down = cuts[0], cuts[1], cuts[2:slots], cuts[slots:]
    got = [along(packed[k], k) for k in range(slots)]
    keyval = jnp.stack([piece[:, :384] for piece in got])
    kv_pieces = [across(keyval, p) for p in range(plane - 1)]
    halves = (kv_pieces[2][: slots // 2], kv_pieces[1][slots // 2 :])
    kv_pieces.append(across(halves[0], 1))
    kv_pieces.append(across(halves[1], 2))

    firsts = [across(early, p) for p in range(3)]
    last_up = across(firsts[2][:block], 1)
    last_down = across(firsts[1][block:], 2)

    def gather(arrays, turn):
        mine = jnp.concatenate(arrays, axis=0) if len(arrays) > 1 else arrays[0]
        near = [mine, across(mine, 1), across(mine, 2)]
        blocks = mine.shape[0] // block
        split = (blocks + 1) // 2
        ways = (1, 2) if turn == 0 else (2, 1)
        pieces = [[(p, near[p], i) for p in range(3)] for i in range(blocks)]
        for way, lo, hi in ((ways[0], 0, split), (ways[1], split, blocks)):
            if hi > lo:
                far = across(near[3 - way][lo * block : hi * block], way)
                for i in range(lo, hi):
                    pieces[i].append((3, far, i - lo))
        return pieces

    def arrange(pieces):
        arrays = []
        moves = []
        for p, k, array, at in pieces:
            numbers = [i for i, other in enumerate(arrays) if other is array]
            if not numbers:
                numbers = [len(arrays)]
                arrays.append(array)
            moves.append((p, k, numbers[0], at))
        return pl.pallas_call(
            functools.partial(arrange_kernel, tuple(moves), plane, block),
            out_shape=jax.ShapeDtypeStruct((count * block, hidden), jnp.bfloat16),
            in_specs=[smem] + vmem_specs(len(arrays)),
            out_specs=pl.BlockSpec(memory_space=VMEM),
            compiler_params=pltpu.CompilerParams(vmem_limit_bytes=16 * 2**20),
            cost_estimate=pl.CostEstimate(flops=10**8, bytes_accessed=10**6, transcendentals=0),
        )(index, *arrays)

    own_up = [(p, 0, firsts[p], 0) for p in range(3)] + [(3, 0, last_up, 0)]
    own_down = [(p, 0, firsts[p], 1) for p in range(3)] + [(3, 0, last_down, 0)]

    def label(k, pieces):
        return [(p, k, array, at) for p, array, at in pieces]

    moved = [along(both, 1)] + [along(cut, k) for k, cut in zip(range(2, slots), cut_up)]
    group = gather(moved, 0)
    own_up += label(1, group[0])
    own_down += label(1, group[1])
    for k in range(2, slots):
        own_up += label(k, group[k])
    for k, cut in zip(range(2, slots), cut_down):
        own_down += label(k, gather([along(cut, k)], k % 2)[0])
    up = arrange(own_up)
    down = arrange(own_down)

    sequence = count * tokens
    heads = pl.pallas_call(
        functools.partial(attend_kernel, slots, plane, tokens),
        out_shape=(jax.ShapeDtypeStruct((tokens, 192), jnp.bfloat16),) * slots,
        in_specs=[smem] * 3 + vmem_specs(3 + slots + plane),
        out_specs=tuple(vmem_specs(slots)),
        compiler_params=pltpu.CompilerParams(vmem_limit_bytes=24 * 2**20),
                scratch_shapes=[
            VMEM((slots, tokens, 192), jnp.bfloat16),
            VMEM((sequence, 384), jnp.bfloat16),
            VMEM((2 * tokens, sequence), jnp.float32),
            VMEM((slots, tokens, 192), jnp.bfloat16),
        ],
        cost_estimate=pl.CostEstimate(flops=8 * 10**9, bytes_accessed=2 * 10**6, transcendentals=0),
        name="attend",
    )(
        index,
        balance_first,
        balance_second,
        head_gain_first[None],
        head_gain_second[None],
        *got,
        *kv_pieces,
    )
    pieces = [along(heads[k], k) for k in range(slots)]
    row_shape = jax.ShapeDtypeStruct((half, width), jnp.bfloat16)
    own, other = pl.pallas_call(
        functools.partial(project_kernel, slots, half),
        out_shape=(row_shape, row_shape),
        in_specs=[smem] + vmem_specs(slots + 2),
        out_specs=tuple(vmem_specs(2)),
        scratch_shapes=[VMEM((slots, tokens, 192), jnp.bfloat16)],
        compiler_params=pltpu.CompilerParams(vmem_limit_bytes=16 * 2**20),
                cost_estimate=pl.CostEstimate(flops=2 * 10**9, bytes_accessed=4 * 10**6, transcendentals=0),
        name="project",
    )(index, *pieces, out_first, out_second)
    mixed, normed = pl.pallas_call(
        functools.partial(norm_kernel, half),
        out_shape=(row_shape, row_shape),
        in_specs=[smem] + vmem_specs(4),
        out_specs=tuple(vmem_specs(2)),
        compiler_params=pltpu.CompilerParams(vmem_limit_bytes=8 * 2**20),
                cost_estimate=pl.CostEstimate(flops=10**9, bytes_accessed=10**6, transcendentals=0),
        name="norm",
    )(index, residual, own, swap(other), mlp_gain[None])
    own_rows = [along(normed, k) for k in range(slots)]
    other_rows = [swap(piece) for piece in own_rows]
    group = slots // 2
    part_shape = jax.ShapeDtypeStruct((group, half, width), jnp.bfloat16)
    total = None

    def lift(chosen_slots):
        chosen = [own_rows[k] for k in chosen_slots] + [other_rows[k] for k in chosen_slots]
        return pl.pallas_call(
            lift_kernel,
            out_shape=jax.ShapeDtypeStruct((2 * group * half, hidden), jnp.bfloat16),
            in_specs=vmem_specs(1 + 2 * group),
            out_specs=pl.BlockSpec(memory_space=VMEM),
            scratch_shapes=[VMEM((2 * group * half, width), jnp.bfloat16)],
            compiler_params=pltpu.CompilerParams(vmem_limit_bytes=16 * 2**20),
            cost_estimate=pl.CostEstimate(flops=3 * 10**9, bytes_accessed=10**6, transcendentals=0),
        )(up, *chosen)

    def lower(active):
        return pl.pallas_call(
            lower_kernel,
            out_shape=(part_shape, part_shape),
            in_specs=vmem_specs(2),
            out_specs=tuple(vmem_specs(2)),
            compiler_params=pltpu.CompilerParams(vmem_limit_bytes=16 * 2**20),
            cost_estimate=pl.CostEstimate(flops=3 * 10**9, bytes_accessed=10**6, transcendentals=0),
        )(active, down)

    terms = {}
    for chosen in (list(range(1, slots, 2)), list(range(slots - 2, -1, -2))):
        own, other = lower(lift(chosen))
        other = swap(other)
        summed = own.astype(jnp.float32) + other.astype(jnp.float32)
        for at, k in enumerate(chosen):
            piece = summed[at]
            terms[k] = piece if k == 0 else along(piece.astype(jnp.bfloat16), k)
    total = terms[0]
    for k in range(1, slots):
        total = total + terms[k].astype(jnp.float32)
    mine = (mixed.astype(jnp.float32) + total).astype(jnp.bfloat16)
    theirs = swap(mine)
    return jnp.where(
        core == 0, jnp.concatenate([mine, theirs]), jnp.concatenate([theirs, mine])
    )


def dispatch(count, cores, *arguments):
    heads, other_heads = arguments[1].shape[1], arguments[4].shape[1]
    plane = count // heads
    fits = (
        cores == 2
        and heads == other_heads
        and plane == 4
        and plane * heads == count
        and arguments[3].shape[2] == 128
        and arguments[6].shape[2] == 64
    )
    if fits:
        return fast_body(heads, plane, *arguments)
    return body(*arguments)


def plan(mesh):
    return functools.partial(dispatch, mesh.shape["sp"], mesh.shape["tp"])


def solution(mesh):
    in_specs = (
        P("sp", None),
        P("sp", "tp", None),
        P("sp", "tp", None),
        P("sp", "tp", None),
        P("sp", "tp", None),
        P("sp", "tp", None),
        P("sp", "tp", None),
        P("tp"),
        P("tp"),
        P(),
        P(),
        P("tp", None),
        P("tp", None),
        P(),
        P("sp", "tp"),
        P("sp", "tp"),
    )
    out_specs = P("sp", None)
    return jax.shard_map(
        plan(mesh), mesh=mesh, in_specs=in_specs, out_specs=out_specs, check_vma=False
    )
```

```python
import functools
import math

import jax
import jax.numpy as jnp
from jax import lax
from jax.experimental import pallas as pl
from jax.experimental.pallas import tpu as pltpu
from jax.sharding import PartitionSpec as P

DK_A = 64
DK_B = 32


EPSILON = 1e-06
HEAD_SCALE = 0.8


def attend(queries, keys, values, balance, gain, device, head_size):
    tokens = queries.shape[0]
    heads = queries.shape[1]
    seq = keys.shape[0]
    depth = values.shape[2]
    block = math.gcd(512, seq)
    scale = head_size ** (-0.5)
    query_maps = queries.reshape(tokens, heads, 2, head_size)
    key_maps = keys.reshape(seq, heads, 2, head_size)
    first_row = device * tokens
    positions = first_row + jnp.arange(tokens, dtype=jnp.int32)
    needed = (first_row + tokens + block - 1) // block

    def block_scores(number):
        start = number * block
        key_block = lax.dynamic_slice_in_dim(key_maps, start, block, 0)
        scores = (
            jnp.einsum("qhmd,khmd->hmqk", query_maps, key_block, preferred_element_type=jnp.float32)
            * scale
        )
        columns = start + jnp.arange(block, dtype=jnp.int32)
        visible = columns[None, :] <= positions[:, None]
        return (jnp.where(visible, scores, -jnp.inf), start)

    def statistics(number, carry):
        highest, total = carry
        scores, _ = block_scores(number)
        fresh = jnp.maximum(highest, jnp.max(scores, axis=-1, keepdims=True))
        total = total * jnp.exp(highest - fresh) + jnp.sum(
            jnp.exp(scores - fresh), axis=-1, keepdims=True
        )
        return (fresh, total)

    start_high = jnp.full((heads, 2, tokens, 1), -jnp.inf, jnp.float32)
    start_total = jnp.zeros((heads, 2, tokens, 1), jnp.float32)
    highest, total = lax.fori_loop(0, needed, statistics, (start_high, start_total))

    def accumulate(number, result):
        scores, start = block_scores(number)
        probs = jnp.exp(scores - highest) / total
        mixed = (probs[:, 0] - balance[:, None, None] * probs[:, 1]).astype(jnp.bfloat16)
        value_block = lax.dynamic_slice_in_dim(values, start, block, 0)
        return result + jnp.einsum(
            "hqk,khe->qhe", mixed, value_block, preferred_element_type=jnp.float32
        )

    summed = lax.fori_loop(0, needed, accumulate, jnp.zeros((tokens, heads, depth), jnp.float32))
    power = jnp.mean(summed * summed, axis=-1, keepdims=True)
    normed = summed * lax.rsqrt(power + EPSILON) * gain * HEAD_SCALE
    return normed.astype(jnp.bfloat16).reshape(tokens, heads * depth)


def body(
    residual,
    query_first,
    key_first,
    value_first,
    query_second,
    key_second,
    value_second,
    balance_first,
    balance_second,
    head_gain_first,
    head_gain_second,
    out_first,
    out_second,
    mlp_gain,
    up_weight,
    down_weight,
):
    device = lax.axis_index("sp")
    keys_first, values_first, keys_second, values_second = (
        lax.all_gather(key_first, "sp", axis=0, tiled=True),
        lax.all_gather(value_first, "sp", axis=0, tiled=True),
        lax.all_gather(key_second, "sp", axis=0, tiled=True),
        lax.all_gather(value_second, "sp", axis=0, tiled=True),
    )
    heads_first = attend(
        query_first, keys_first, values_first, balance_first, head_gain_first, device, DK_A
    )
    heads_second = attend(
        query_second, keys_second, values_second, balance_second, head_gain_second, device, DK_B
    )
    head_term = jnp.dot(heads_first, out_first, preferred_element_type=jnp.float32) + jnp.dot(
        heads_second, out_second, preferred_element_type=jnp.float32
    )
    head_total = lax.psum(head_term.astype(jnp.bfloat16), "tp").astype(jnp.float32)
    mixed = (residual.astype(jnp.float32) + head_total).astype(jnp.bfloat16)
    mixed_float = mixed.astype(jnp.float32)
    power = jnp.mean(mixed_float * mixed_float, axis=-1, keepdims=True)
    normed = (mixed_float * lax.rsqrt(power + EPSILON) * mlp_gain).astype(jnp.bfloat16)
    up_whole, down_whole = (
        lax.all_gather(up_weight, "sp", axis=0, tiled=True),
        lax.all_gather(down_weight, "sp", axis=0, tiled=True),
    )
    lifted = jnp.dot(normed, up_whole, preferred_element_type=jnp.float32)
    active = jax.nn.relu(lifted)
    hidden = (active * active).astype(jnp.bfloat16)
    down_term = lax.dot_general(
        hidden, down_whole, (((1,), (1,)), ((), ())), preferred_element_type=jnp.float32
    )
    added = lax.psum(down_term.astype(jnp.bfloat16), "tp").astype(jnp.float32)
    return (mixed_float + added).astype(jnp.bfloat16)


VMEM = pltpu.VMEM
SMEM = pltpu.SMEM
DIRECT = 0.375


def vmem_specs(count):
    return [pl.BlockSpec(memory_space=VMEM)] * count


def pack_kernel(slots, index, *refs):
    sources, outs, held = refs[:6], refs[6 : 6 + slots], refs[6 + slots : -2]
    packed, arrived = refs[-2:]
    copies = [
        pltpu.make_async_copy(source, target, arrived.at[i])
        for i, (source, target) in enumerate(zip(sources, held))
    ]
    for copy in copies:
        copy.start()
    for copy in copies:
        copy.wait()
    key_a, key_b, value_b, value_a, query_a, query_b = held
    for head in range(slots):
        packed[head, :, 0:128] = key_a[:, head, :]
        packed[head, :, 128:192] = key_b[head].T
        packed[head, :, 192:256] = value_b[head].T
        packed[head, :, 256:384] = value_a[:, head, :]
        packed[head, :, 384:512] = query_a[:, head, :]
        packed[head, :, 512:576] = query_b[head].T
    for k in range(slots):
        outs[k][...] = packed[index[0] ^ k]


def cut_kernel(slots, width, index, *refs):
    weights, pairs, ups, downs = refs[:2], refs[2:4], refs[4 : 2 + slots], refs[2 + slots : -1]
    arrived = refs[-1]
    block = weights[0].shape[0]
    copies = []
    for i, (weight, pieces) in enumerate(zip(weights, (ups, downs))):
        for k in range(slots):
            place = pl.ds(pl.multiple_of((index[0] ^ k) * width, width), width)
            target = pairs[k].at[pl.ds(i * block, block), :] if k < 2 else pieces[k - 2]
            copies.append(
                pltpu.make_async_copy(weight.at[:, place], target, arrived.at[i * slots + k])
            )
    for copy in copies:
        copy.start()
    for copy in copies:
        copy.wait()


def attend_kernel(slots, plane, tokens, index, balance_a, balance_b, gain_a, gain_b, *refs):
    queries, kv_pieces = refs[:slots], refs[slots : slots + plane + 1]
    outs = refs[slots + plane + 1 : 2 * slots + plane + 1]
    query, keyval, scores, out = refs[2 * slots + plane + 1 :]
    z, g = index[0], index[1]
    wide = plane * tokens
    for k in range(slots):
        query[z ^ k] = queries[k][:, 384:576]
        for p in range(plane):
            start = pl.multiple_of(((z ^ k) * plane + (g ^ p)) * tokens, tokens)
            if p < plane - 1:
                keyval[pl.ds(start, tokens), :] = kv_pieces[p][k]
            else:
                part = slots // 2
                keyval[pl.ds(start, tokens), :] = kv_pieces[p + k // part][k % part]
    lane = lax.broadcasted_iota(jnp.int32, (tokens, 128), 1)
    row = lax.broadcasted_iota(jnp.int32, (2 * tokens, wide), 0) % tokens
    column = lax.broadcasted_iota(jnp.int32, (2 * tokens, wide), 1)
    visible = column <= row + g * tokens

    def group(number, place, size, key_lo, value_lo, balance):
        packed = query[number][:, place : place + 2 * size]
        if 2 * size < 128:
            packed = jnp.concatenate(
                [packed, jnp.zeros((tokens, 128 - 2 * size), packed.dtype)], axis=1
            )
        zero = jnp.zeros_like(packed)
        both = jnp.concatenate(
            [jnp.where(lane < size, packed, zero), jnp.where(lane >= size, packed, zero)], axis=0
        )
        factor = size ** (-0.5) * math.log2(math.e)
        highest = None
        for c in range(number + 1):
            part = lax.dot_general(
                both,
                keyval[c * wide : (c + 1) * wide, key_lo : key_lo + 128],
                (((1,), (1,)), ((), ())),
                preferred_element_type=jnp.float32,
            )
            if c == number:
                part = jnp.where(visible, part, -jnp.inf)
            scores[:, c * wide : (c + 1) * wide] = part
            top = jnp.max(part, axis=1, keepdims=True)
            highest = top if highest is None else jnp.maximum(highest, top)
        total = jnp.zeros((2 * tokens, 1), jnp.float32)
        for c in range(number + 1):
            part = jnp.exp2((scores[:, c * wide : (c + 1) * wide] - highest) * factor)
            scores[:, c * wide : (c + 1) * wide] = part
            total = total + jnp.sum(part, axis=1, keepdims=True)
        share = 1.0 / total
        first, second = share[:tokens], share[tokens:] * balance
        summed = jnp.zeros((tokens, 128), jnp.float32)
        for c in range(number + 1):
            span = slice(c * wide, (c + 1) * wide)
            weights = (scores[:tokens, span] * first - scores[tokens:, span] * second).astype(
                jnp.bfloat16
            )
            summed = summed + jnp.dot(
                weights, keyval[span, value_lo : value_lo + 128], preferred_element_type=jnp.float32
            )
        return summed

    def normed(summed, gain):
        power = jnp.mean(summed * summed, axis=-1, keepdims=True)
        return (summed * lax.rsqrt(power + EPSILON) * gain[...] * HEAD_SCALE).astype(jnp.bfloat16)

    for number in range(slots):
        summed = group(number, 0, DK_A, 0, 256, balance_a[z])
        out[number, :, 0:128] = normed(summed, gain_a)
        summed = group(number, 128, DK_B, 128, 128, balance_b[z])[:, 64:128]
        out[number, :, 128:192] = normed(summed, gain_b)
    for k in range(slots):
        outs[k][...] = out[z ^ k]


def project_kernel(slots, half, index, *refs):
    pieces, out_a, out_b, own, other, left = (
        refs[:slots],
        refs[slots],
        refs[slots + 1],
        refs[slots + 2],
        refs[slots + 3],
        refs[slots + 4],
    )
    z, core = index[0], index[2]
    mine = pl.multiple_of(core * half, half)
    theirs = pl.multiple_of((1 - core) * half, half)
    for k in range(slots):
        left[k, :half] = pieces[k][pl.ds(mine, half), :]
        left[k, half:] = pieces[k][pl.ds(theirs, half), :]
    tile = 512
    for n in range(out_a.shape[1] // tile):
        span = slice(n * tile, (n + 1) * tile)
        total = jnp.zeros((2 * half, tile), jnp.float32)
        for k in range(slots):
            head = z ^ k
            total += jnp.dot(
                left[k, :, 0:128],
                out_a[pl.ds(pl.multiple_of(head * 128, 128), 128), span],
                preferred_element_type=jnp.float32,
            )
            total += jnp.dot(
                left[k, :, 128:192],
                out_b[pl.ds(pl.multiple_of(head * 64, 64), 64), span],
                preferred_element_type=jnp.float32,
            )
        total = total.astype(jnp.bfloat16)
        own[:, span] = total[:half]
        other[:, span] = total[half:]


def norm_kernel(half, index, residual, own, other, gain, mixed, normed):
    mine = pl.multiple_of(index[2] * half, half)
    total = own[...].astype(jnp.float32) + other[...].astype(jnp.float32)
    rounded = (residual[pl.ds(mine, half), :].astype(jnp.float32) + total).astype(jnp.bfloat16)
    mixed[...] = rounded
    value = rounded.astype(jnp.float32)
    power = jnp.mean(value * value, axis=-1, keepdims=True)
    normed[...] = (value * lax.rsqrt(power + EPSILON) * gain[...]).astype(jnp.bfloat16)


def arrange_kernel(moves, plane, block, index, *refs):
    out = refs[-1]
    z, g = index[0], index[1]
    for p, k, number, at in moves:
        place = pl.multiple_of(((z ^ k) * plane + (g ^ p)) * block, block)
        out[pl.ds(place, block), :] = refs[number][at * block : (at + 1) * block, :]


def lift_kernel(up, *refs):
    rows, hidden, left = refs[:-2], refs[-2], refs[-1]
    half = rows[0].shape[0]
    for r, piece in enumerate(rows):
        left[r * half : (r + 1) * half, :] = piece[...]
    tile = 256
    for n in range(up.shape[1] // tile):
        span = slice(n * tile, (n + 1) * tile)
        active = jnp.maximum(
            jnp.dot(left[...], up[:, span], preferred_element_type=jnp.float32), 0.0
        )
        hidden[:, span] = (active * active).astype(jnp.bfloat16)


def lower_kernel(hidden, down, own, other):
    count, half, width = own.shape
    tile = 512
    for n in range(width // tile):
        span = slice(n * tile, (n + 1) * tile)
        part = lax.dot_general(
            hidden[...],
            down[span, :],
            (((1,), (1,)), ((), ())),
            preferred_element_type=jnp.float32,
        ).astype(jnp.bfloat16)
        for r in range(count):
            rest = (r + count) * half
            own[r, :, span] = part[r * half : (r + 1) * half]
            other[r, :, span] = part[rest : rest + half]


def fast_body(slots, plane, *arguments):
    (
        residual,
        query_first,
        key_first,
        value_first,
        query_second,
        key_second,
        value_second,
        balance_first,
        balance_second,
        head_gain_first,
        head_gain_second,
        out_first,
        out_second,
        mlp_gain,
        up_weight,
        down_weight,
    ) = arguments
    count = slots * plane
    tokens, width = residual.shape
    half = tokens // 2
    device, core = lax.axis_index("sp"), lax.axis_index("tp")
    z, g = device // plane, device % plane
    index = jnp.stack([z, g, core]).astype(jnp.int32)

    def along(value, k):
        if k == 0:
            return value
        return lax.ppermute(
            value, "sp", [(i, (i // plane ^ k) * plane + i % plane) for i in range(count)]
        )

    def across(value, k):
        if k == 0:
            return value
        return lax.ppermute(value, "sp", [(i, i ^ k) for i in range(count)])

    def swap(value):
        return lax.ppermute(value, "tp", [(0, 1), (1, 0)])

    smem = pl.BlockSpec(memory_space=SMEM)
    hidden = up_weight.shape[1] // slots
    block = up_weight.shape[0]
    sources = (
        key_first,
        key_second.transpose(1, 2, 0),
        value_second.transpose(1, 2, 0),
        value_first,
        query_first,
        query_second.transpose(1, 2, 0),
    )
    packed = pl.pallas_call(
        functools.partial(pack_kernel, slots),
        out_shape=(jax.ShapeDtypeStruct((tokens, 576), jnp.bfloat16),) * slots,
        in_specs=[smem] + [pl.BlockSpec(memory_space=pltpu.HBM)] * 6,
        out_specs=tuple(vmem_specs(slots)),
        scratch_shapes=[VMEM(source.shape, jnp.bfloat16) for source in sources]
        + [VMEM((slots, tokens, 576), jnp.bfloat16), pltpu.SemaphoreType.DMA((6,))],
        cost_estimate=pl.CostEstimate(flops=10**8, bytes_accessed=10**6, transcendentals=0),
        name="pack",
    )(index, *sources)
    piece_shape = jax.ShapeDtypeStruct((block, hidden), jnp.bfloat16)
    cuts = pl.pallas_call(
        functools.partial(cut_kernel, slots, hidden),
        out_shape=(jax.ShapeDtypeStruct((2 * block, hidden), jnp.bfloat16),) * 2
        + (piece_shape,) * (2 * slots - 4),
        in_specs=[smem] + [pl.BlockSpec(memory_space=pltpu.HBM)] * 2,
        out_specs=tuple(vmem_specs(2 * slots - 2)),
        scratch_shapes=[pltpu.SemaphoreType.DMA((2 * slots,))],
        cost_estimate=pl.CostEstimate(flops=10**8, bytes_accessed=10**6, transcendentals=0),
        name="cut",
    )(index, up_weight, down_weight)
    early, both, cut_up, cut_down = cuts[0], cuts[1], cuts[2:slots], cuts[slots:]
    got = [along(packed[k], k) for k in range(slots)]
    keyval = jnp.stack([piece[:, :384] for piece in got])
    kv_pieces = [across(keyval, p) for p in range(plane - 1)]
    halves = (kv_pieces[2][: slots // 2], kv_pieces[1][slots // 2 :])
    kv_pieces.append(across(halves[0], 1))
    kv_pieces.append(across(halves[1], 2))

    firsts = [across(early, p) for p in range(3)]
    last_up = across(firsts[2][:block], 1)
    last_down = across(firsts[1][block:], 2)

    def gather(arrays, turn):
        mine = jnp.concatenate(arrays, axis=0) if len(arrays) > 1 else arrays[0]
        near = [mine, across(mine, 1), across(mine, 2)]
        blocks = mine.shape[0] // block
        split = (blocks + 1) // 2
        ways = (1, 2) if turn == 0 else (2, 1)
        pieces = [[(p, near[p], i) for p in range(3)] for i in range(blocks)]
        for way, lo, hi in ((ways[0], 0, split), (ways[1], split, blocks)):
            if hi > lo:
                far = across(near[3 - way][lo * block : hi * block], way)
                for i in range(lo, hi):
                    pieces[i].append((3, far, i - lo))
        return pieces

    def arrange(pieces):
        arrays = []
        moves = []
        for p, k, array, at in pieces:
            numbers = [i for i, other in enumerate(arrays) if other is array]
            if not numbers:
                numbers = [len(arrays)]
                arrays.append(array)
            moves.append((p, k, numbers[0], at))
        return pl.pallas_call(
            functools.partial(arrange_kernel, tuple(moves), plane, block),
            out_shape=jax.ShapeDtypeStruct((count * block, hidden), jnp.bfloat16),
            in_specs=[smem] + vmem_specs(len(arrays)),
            out_specs=pl.BlockSpec(memory_space=VMEM),
            compiler_params=pltpu.CompilerParams(vmem_limit_bytes=16 * 2**20),
            cost_estimate=pl.CostEstimate(flops=10**8, bytes_accessed=10**6, transcendentals=0),
        )(index, *arrays)

    own_up = [(p, 0, firsts[p], 0) for p in range(3)] + [(3, 0, last_up, 0)]
    own_down = [(p, 0, firsts[p], 1) for p in range(3)] + [(3, 0, last_down, 0)]

    def label(k, pieces):
        return [(p, k, array, at) for p, array, at in pieces]

    moved = [along(both, 1)] + [along(cut, k) for k, cut in zip(range(2, slots), cut_up)]
    group = gather(moved, 0)
    own_up += label(1, group[0])
    own_down += label(1, group[1])
    for k in range(2, slots):
        own_up += label(k, group[k])
    for k, cut in zip(range(2, slots), cut_down):
        own_down += label(k, gather([along(cut, k)], k % 2)[0])
    up = arrange(own_up)
    down = arrange(own_down)

    sequence = count * tokens
    heads = pl.pallas_call(
        functools.partial(attend_kernel, slots, plane, tokens),
        out_shape=(jax.ShapeDtypeStruct((tokens, 192), jnp.bfloat16),) * slots,
        in_specs=[smem] * 3 + vmem_specs(3 + slots + plane),
        out_specs=tuple(vmem_specs(slots)),
        compiler_params=pltpu.CompilerParams(vmem_limit_bytes=24 * 2**20),
                scratch_shapes=[
            VMEM((slots, tokens, 192), jnp.bfloat16),
            VMEM((sequence, 384), jnp.bfloat16),
            VMEM((2 * tokens, sequence), jnp.float32),
            VMEM((slots, tokens, 192), jnp.bfloat16),
        ],
        cost_estimate=pl.CostEstimate(flops=8 * 10**9, bytes_accessed=2 * 10**6, transcendentals=0),
        name="attend",
    )(
        index,
        balance_first,
        balance_second,
        head_gain_first[None],
        head_gain_second[None],
        *got,
        *kv_pieces,
    )
    pieces = [along(heads[k], k) for k in range(slots)]
    row_shape = jax.ShapeDtypeStruct((half, width), jnp.bfloat16)
    own, other = pl.pallas_call(
        functools.partial(project_kernel, slots, half),
        out_shape=(row_shape, row_shape),
        in_specs=[smem] + vmem_specs(slots + 2),
        out_specs=tuple(vmem_specs(2)),
        scratch_shapes=[VMEM((slots, tokens, 192), jnp.bfloat16)],
        compiler_params=pltpu.CompilerParams(vmem_limit_bytes=16 * 2**20),
                cost_estimate=pl.CostEstimate(flops=2 * 10**9, bytes_accessed=4 * 10**6, transcendentals=0),
        name="project",
    )(index, *pieces, out_first, out_second)
    mixed, normed = pl.pallas_call(
        functools.partial(norm_kernel, half),
        out_shape=(row_shape, row_shape),
        in_specs=[smem] + vmem_specs(4),
        out_specs=tuple(vmem_specs(2)),
        compiler_params=pltpu.CompilerParams(vmem_limit_bytes=8 * 2**20),
                cost_estimate=pl.CostEstimate(flops=10**9, bytes_accessed=10**6, transcendentals=0),
        name="norm",
    )(index, residual, own, swap(other), mlp_gain[None])
    own_rows = [along(normed, k) for k in range(3)]
    own_rows.append(along(own_rows[2], 1))
    other_rows = [swap(piece) for piece in own_rows]
    group = slots // 2
    part_shape = jax.ShapeDtypeStruct((group, half, width), jnp.bfloat16)
    total = None

    def lift(chosen_slots):
        chosen = [own_rows[k] for k in chosen_slots] + [other_rows[k] for k in chosen_slots]
        return pl.pallas_call(
            lift_kernel,
            out_shape=jax.ShapeDtypeStruct((2 * group * half, hidden), jnp.bfloat16),
            in_specs=vmem_specs(1 + 2 * group),
            out_specs=pl.BlockSpec(memory_space=VMEM),
            scratch_shapes=[VMEM((2 * group * half, width), jnp.bfloat16)],
            compiler_params=pltpu.CompilerParams(vmem_limit_bytes=16 * 2**20),
            cost_estimate=pl.CostEstimate(flops=3 * 10**9, bytes_accessed=10**6, transcendentals=0),
        )(up, *chosen)

    def lower(active):
        return pl.pallas_call(
            lower_kernel,
            out_shape=(part_shape, part_shape),
            in_specs=vmem_specs(2),
            out_specs=tuple(vmem_specs(2)),
            compiler_params=pltpu.CompilerParams(vmem_limit_bytes=16 * 2**20),
            cost_estimate=pl.CostEstimate(flops=3 * 10**9, bytes_accessed=10**6, transcendentals=0),
        )(active, down)

    def finish(chosen):
        own, other = lower(lift(chosen))
        other = swap(other)
        summed = own.astype(jnp.float32) + other.astype(jnp.float32)
        return summed[0], summed[1]

    farthest, far = finish((3, 2))
    direct = 128 * round(width * DIRECT / 128)
    sent, far_sent = farthest.astype(jnp.bfloat16), far.astype(jnp.bfloat16)
    passed = along(sent[:, direct:], 1).astype(jnp.float32)
    straight = along(sent[:, :direct], 3).astype(jnp.float32)
    straight = straight + along(far_sent[:, :direct], 2).astype(jnp.float32)
    relayed = along((far[:, direct:] + passed).astype(jnp.bfloat16), 2).astype(jnp.float32)
    near, total = finish((1, 0))
    total = total + along(near.astype(jnp.bfloat16), 1).astype(jnp.float32)
    total = total + jnp.concatenate([straight, relayed], axis=1)
    mine = (mixed.astype(jnp.float32) + total).astype(jnp.bfloat16)
    theirs = swap(mine)
    return jnp.where(
        core == 0, jnp.concatenate([mine, theirs]), jnp.concatenate([theirs, mine])
    )


def dispatch(count, cores, *arguments):
    heads, other_heads = arguments[1].shape[1], arguments[4].shape[1]
    plane = count // heads
    fits = (
        cores == 2
        and heads == other_heads
        and plane == 4
        and heads == 4
        and plane * heads == count
        and arguments[3].shape[2] == 128
        and arguments[6].shape[2] == 64
    )
    if fits:
        return fast_body(heads, plane, *arguments)
    return body(*arguments)


def plan(mesh):
    return functools.partial(dispatch, mesh.shape["sp"], mesh.shape["tp"])


def solution(mesh):
    in_specs = (
        P("sp", None),
        P("sp", "tp", None),
        P("sp", "tp", None),
        P("sp", "tp", None),
        P("sp", "tp", None),
        P("sp", "tp", None),
        P("sp", "tp", None),
        P("tp"),
        P("tp"),
        P(),
        P(),
        P("tp", None),
        P("tp", None),
        P(),
        P("sp", "tp"),
        P("sp", "tp"),
    )
    out_specs = P("sp", None)
    return jax.shard_map(
        plan(mesh), mesh=mesh, in_specs=in_specs, out_specs=out_specs, check_vma=False
    )
```

```python
import functools
import math

import jax
import jax.numpy as jnp
from jax import lax
from jax.experimental import pallas as pl
from jax.experimental.pallas import tpu as pltpu
from jax.sharding import PartitionSpec as P

DK_A = 64
DK_B = 32


EPSILON = 1e-06
HEAD_SCALE = 0.8


def attend(queries, keys, values, balance, gain, device, head_size):
    tokens = queries.shape[0]
    heads = queries.shape[1]
    seq = keys.shape[0]
    depth = values.shape[2]
    block = math.gcd(512, seq)
    scale = head_size ** (-0.5)
    query_maps = queries.reshape(tokens, heads, 2, head_size)
    key_maps = keys.reshape(seq, heads, 2, head_size)
    first_row = device * tokens
    positions = first_row + jnp.arange(tokens, dtype=jnp.int32)
    needed = (first_row + tokens + block - 1) // block

    def block_scores(number):
        start = number * block
        key_block = lax.dynamic_slice_in_dim(key_maps, start, block, 0)
        scores = (
            jnp.einsum("qhmd,khmd->hmqk", query_maps, key_block, preferred_element_type=jnp.float32)
            * scale
        )
        columns = start + jnp.arange(block, dtype=jnp.int32)
        visible = columns[None, :] <= positions[:, None]
        return (jnp.where(visible, scores, -jnp.inf), start)

    def statistics(number, carry):
        highest, total = carry
        scores, _ = block_scores(number)
        fresh = jnp.maximum(highest, jnp.max(scores, axis=-1, keepdims=True))
        total = total * jnp.exp(highest - fresh) + jnp.sum(
            jnp.exp(scores - fresh), axis=-1, keepdims=True
        )
        return (fresh, total)

    start_high = jnp.full((heads, 2, tokens, 1), -jnp.inf, jnp.float32)
    start_total = jnp.zeros((heads, 2, tokens, 1), jnp.float32)
    highest, total = lax.fori_loop(0, needed, statistics, (start_high, start_total))

    def accumulate(number, result):
        scores, start = block_scores(number)
        probs = jnp.exp(scores - highest) / total
        mixed = (probs[:, 0] - balance[:, None, None] * probs[:, 1]).astype(jnp.bfloat16)
        value_block = lax.dynamic_slice_in_dim(values, start, block, 0)
        return result + jnp.einsum(
            "hqk,khe->qhe", mixed, value_block, preferred_element_type=jnp.float32
        )

    summed = lax.fori_loop(0, needed, accumulate, jnp.zeros((tokens, heads, depth), jnp.float32))
    power = jnp.mean(summed * summed, axis=-1, keepdims=True)
    normed = summed * lax.rsqrt(power + EPSILON) * gain * HEAD_SCALE
    return normed.astype(jnp.bfloat16).reshape(tokens, heads * depth)


def body(
    residual,
    query_first,
    key_first,
    value_first,
    query_second,
    key_second,
    value_second,
    balance_first,
    balance_second,
    head_gain_first,
    head_gain_second,
    out_first,
    out_second,
    mlp_gain,
    up_weight,
    down_weight,
):
    device = lax.axis_index("sp")
    keys_first, values_first, keys_second, values_second = (
        lax.all_gather(key_first, "sp", axis=0, tiled=True),
        lax.all_gather(value_first, "sp", axis=0, tiled=True),
        lax.all_gather(key_second, "sp", axis=0, tiled=True),
        lax.all_gather(value_second, "sp", axis=0, tiled=True),
    )
    heads_first = attend(
        query_first, keys_first, values_first, balance_first, head_gain_first, device, DK_A
    )
    heads_second = attend(
        query_second, keys_second, values_second, balance_second, head_gain_second, device, DK_B
    )
    head_term = jnp.dot(heads_first, out_first, preferred_element_type=jnp.float32) + jnp.dot(
        heads_second, out_second, preferred_element_type=jnp.float32
    )
    head_total = lax.psum(head_term.astype(jnp.bfloat16), "tp").astype(jnp.float32)
    mixed = (residual.astype(jnp.float32) + head_total).astype(jnp.bfloat16)
    mixed_float = mixed.astype(jnp.float32)
    power = jnp.mean(mixed_float * mixed_float, axis=-1, keepdims=True)
    normed = (mixed_float * lax.rsqrt(power + EPSILON) * mlp_gain).astype(jnp.bfloat16)
    up_whole, down_whole = (
        lax.all_gather(up_weight, "sp", axis=0, tiled=True),
        lax.all_gather(down_weight, "sp", axis=0, tiled=True),
    )
    lifted = jnp.dot(normed, up_whole, preferred_element_type=jnp.float32)
    active = jax.nn.relu(lifted)
    hidden = (active * active).astype(jnp.bfloat16)
    down_term = lax.dot_general(
        hidden, down_whole, (((1,), (1,)), ((), ())), preferred_element_type=jnp.float32
    )
    added = lax.psum(down_term.astype(jnp.bfloat16), "tp").astype(jnp.float32)
    return (mixed_float + added).astype(jnp.bfloat16)


VMEM = pltpu.VMEM
SMEM = pltpu.SMEM
DIRECT = 0.25


def vmem_specs(count):
    return [pl.BlockSpec(memory_space=VMEM)] * count


def pack_kernel(slots, index, *refs):
    sources, outs, held = refs[:6], refs[6 : 6 + slots], refs[6 + slots : -2]
    packed, arrived = refs[-2:]
    copies = [
        pltpu.make_async_copy(source, target, arrived.at[i])
        for i, (source, target) in enumerate(zip(sources, held))
    ]
    for copy in copies:
        copy.start()
    for copy in copies:
        copy.wait()
    key_a, key_b, value_b, value_a, query_a, query_b = held
    for head in range(slots):
        packed[head, :, 0:128] = key_a[:, head, :]
        packed[head, :, 128:192] = key_b[head].T
        packed[head, :, 192:256] = value_b[head].T
        packed[head, :, 256:384] = value_a[:, head, :]
        packed[head, :, 384:512] = query_a[:, head, :]
        packed[head, :, 512:576] = query_b[head].T
    for k in range(slots):
        outs[k][...] = packed[index[0] ^ k]


def cut_kernel(slots, width, index, *refs):
    weights, pairs, lasts = refs[:2], refs[2 : 1 + slots], refs[1 + slots : -1]
    arrived = refs[-1]
    block = weights[0].shape[0]
    copies = []
    for i, (weight, last) in enumerate(zip(weights, lasts)):
        for k in range(slots):
            place = pl.ds(pl.multiple_of((index[0] ^ k) * width, width), width)
            target = last if k == slots - 1 else pairs[k].at[pl.ds(i * block, block), :]
            copies.append(
                pltpu.make_async_copy(weight.at[:, place], target, arrived.at[i * slots + k])
            )
    for copy in copies:
        copy.start()
    for copy in copies:
        copy.wait()


def attend_kernel(slots, plane, tokens, index, balance_a, balance_b, gain_a, gain_b, *refs):
    queries, kv_pieces = refs[:slots], refs[slots : slots + plane + 1]
    outs = refs[slots + plane + 1 : 2 * slots + plane + 1]
    query, keyval, scores, out = refs[2 * slots + plane + 1 :]
    z, g = index[0], index[1]
    wide = plane * tokens
    for k in range(slots):
        query[z ^ k] = queries[k][:, 384:576]
        for p in range(plane):
            start = pl.multiple_of(((z ^ k) * plane + (g ^ p)) * tokens, tokens)
            if p < plane - 1:
                keyval[pl.ds(start, tokens), :] = kv_pieces[p][k]
            else:
                part = slots // 2
                keyval[pl.ds(start, tokens), :] = kv_pieces[p + k // part][k % part]
    lane = lax.broadcasted_iota(jnp.int32, (tokens, 128), 1)
    row = lax.broadcasted_iota(jnp.int32, (2 * tokens, wide), 0) % tokens
    column = lax.broadcasted_iota(jnp.int32, (2 * tokens, wide), 1)
    visible = column <= row + g * tokens

    def group(number, place, size, key_lo, value_lo, balance):
        packed = query[number][:, place : place + 2 * size]
        if 2 * size < 128:
            packed = jnp.concatenate(
                [packed, jnp.zeros((tokens, 128 - 2 * size), packed.dtype)], axis=1
            )
        zero = jnp.zeros_like(packed)
        both = jnp.concatenate(
            [jnp.where(lane < size, packed, zero), jnp.where(lane >= size, packed, zero)], axis=0
        )
        factor = size ** (-0.5) * math.log2(math.e)
        highest = None
        for c in range(number + 1):
            part = lax.dot_general(
                both,
                keyval[c * wide : (c + 1) * wide, key_lo : key_lo + 128],
                (((1,), (1,)), ((), ())),
                preferred_element_type=jnp.float32,
            )
            if c == number:
                part = jnp.where(visible, part, -jnp.inf)
            scores[:, c * wide : (c + 1) * wide] = part
            top = jnp.max(part, axis=1, keepdims=True)
            highest = top if highest is None else jnp.maximum(highest, top)
        total = jnp.zeros((2 * tokens, 1), jnp.float32)
        for c in range(number + 1):
            part = jnp.exp2((scores[:, c * wide : (c + 1) * wide] - highest) * factor)
            scores[:, c * wide : (c + 1) * wide] = part
            total = total + jnp.sum(part, axis=1, keepdims=True)
        share = 1.0 / total
        first, second = share[:tokens], share[tokens:] * balance
        summed = jnp.zeros((tokens, 128), jnp.float32)
        for c in range(number + 1):
            span = slice(c * wide, (c + 1) * wide)
            weights = (scores[:tokens, span] * first - scores[tokens:, span] * second).astype(
                jnp.bfloat16
            )
            summed = summed + jnp.dot(
                weights, keyval[span, value_lo : value_lo + 128], preferred_element_type=jnp.float32
            )
        return summed

    def normed(summed, gain):
        power = jnp.mean(summed * summed, axis=-1, keepdims=True)
        return (summed * lax.rsqrt(power + EPSILON) * gain[...] * HEAD_SCALE).astype(jnp.bfloat16)

    for number in range(slots):
        summed = group(number, 0, DK_A, 0, 256, balance_a[z])
        out[number, :, 0:128] = normed(summed, gain_a)
        summed = group(number, 128, DK_B, 128, 128, balance_b[z])[:, 64:128]
        out[number, :, 128:192] = normed(summed, gain_b)
    for k in range(slots):
        outs[k][...] = out[z ^ k]


def project_kernel(slots, half, index, *refs):
    pieces, out_a, out_b, own, other, left = (
        refs[:slots],
        refs[slots],
        refs[slots + 1],
        refs[slots + 2],
        refs[slots + 3],
        refs[slots + 4],
    )
    z, core = index[0], index[2]
    mine = pl.multiple_of(core * half, half)
    theirs = pl.multiple_of((1 - core) * half, half)
    for k in range(slots):
        left[k, :half] = pieces[k][pl.ds(mine, half), :]
        left[k, half:] = pieces[k][pl.ds(theirs, half), :]
    tile = 512
    for n in range(out_a.shape[1] // tile):
        span = slice(n * tile, (n + 1) * tile)
        total = jnp.zeros((2 * half, tile), jnp.float32)
        for k in range(slots):
            head = z ^ k
            total += jnp.dot(
                left[k, :, 0:128],
                out_a[pl.ds(pl.multiple_of(head * 128, 128), 128), span],
                preferred_element_type=jnp.float32,
            )
            total += jnp.dot(
                left[k, :, 128:192],
                out_b[pl.ds(pl.multiple_of(head * 64, 64), 64), span],
                preferred_element_type=jnp.float32,
            )
        total = total.astype(jnp.bfloat16)
        own[:, span] = total[:half]
        other[:, span] = total[half:]


def norm_kernel(half, index, residual, own, other, gain, mixed, normed):
    mine = pl.multiple_of(index[2] * half, half)
    total = own[...].astype(jnp.float32) + other[...].astype(jnp.float32)
    rounded = (residual[pl.ds(mine, half), :].astype(jnp.float32) + total).astype(jnp.bfloat16)
    mixed[...] = rounded
    value = rounded.astype(jnp.float32)
    power = jnp.mean(value * value, axis=-1, keepdims=True)
    normed[...] = (value * lax.rsqrt(power + EPSILON) * gain[...]).astype(jnp.bfloat16)


def arrange_kernel(moves, plane, block, index, *refs):
    out = refs[-1]
    z, g = index[0], index[1]
    for p, k, number, source, target, rows in moves:
        place = ((z ^ k) * plane + (g ^ p)) * block + target
        out[pl.ds(pl.multiple_of(place, rows), rows), :] = refs[number][source : source + rows, :]


def lift_kernel(up, *refs):
    rows, hidden, left = refs[:-2], refs[-2], refs[-1]
    half = rows[0].shape[0]
    for r, piece in enumerate(rows):
        left[r * half : (r + 1) * half, :] = piece[...]
    tile = 256
    for n in range(up.shape[1] // tile):
        span = slice(n * tile, (n + 1) * tile)
        active = jnp.maximum(
            jnp.dot(left[...], up[:, span], preferred_element_type=jnp.float32), 0.0
        )
        hidden[:, span] = (active * active).astype(jnp.bfloat16)


def lower_kernel(hidden, down, own, other):
    count, half, width = own.shape
    tile = 512
    for n in range(width // tile):
        span = slice(n * tile, (n + 1) * tile)
        part = lax.dot_general(
            hidden[...],
            down[span, :],
            (((1,), (1,)), ((), ())),
            preferred_element_type=jnp.float32,
        ).astype(jnp.bfloat16)
        for r in range(count):
            rest = (r + count) * half
            own[r, :, span] = part[r * half : (r + 1) * half]
            other[r, :, span] = part[rest : rest + half]


def fast_body(slots, plane, *arguments):
    (
        residual,
        query_first,
        key_first,
        value_first,
        query_second,
        key_second,
        value_second,
        balance_first,
        balance_second,
        head_gain_first,
        head_gain_second,
        out_first,
        out_second,
        mlp_gain,
        up_weight,
        down_weight,
    ) = arguments
    count = slots * plane
    tokens, width = residual.shape
    half = tokens // 2
    device, core = lax.axis_index("sp"), lax.axis_index("tp")
    z, g = device // plane, device % plane
    index = jnp.stack([z, g, core]).astype(jnp.int32)

    def along(value, k):
        if k == 0:
            return value
        return lax.ppermute(
            value, "sp", [(i, (i // plane ^ k) * plane + i % plane) for i in range(count)]
        )

    def across(value, k):
        if k == 0:
            return value
        return lax.ppermute(value, "sp", [(i, i ^ k) for i in range(count)])

    def swap(value):
        return lax.ppermute(value, "tp", [(0, 1), (1, 0)])

    smem = pl.BlockSpec(memory_space=SMEM)
    hidden = up_weight.shape[1] // slots
    block = up_weight.shape[0]
    sources = (
        key_first,
        key_second.transpose(1, 2, 0),
        value_second.transpose(1, 2, 0),
        value_first,
        query_first,
        query_second.transpose(1, 2, 0),
    )
    packed = pl.pallas_call(
        functools.partial(pack_kernel, slots),
        out_shape=(jax.ShapeDtypeStruct((tokens, 576), jnp.bfloat16),) * slots,
        in_specs=[smem] + [pl.BlockSpec(memory_space=pltpu.HBM)] * 6,
        out_specs=tuple(vmem_specs(slots)),
        scratch_shapes=[VMEM(source.shape, jnp.bfloat16) for source in sources]
        + [VMEM((slots, tokens, 576), jnp.bfloat16), pltpu.SemaphoreType.DMA((6,))],
        cost_estimate=pl.CostEstimate(flops=10**8, bytes_accessed=10**6, transcendentals=0),
        name="pack",
    )(index, *sources)
    piece_shape = jax.ShapeDtypeStruct((block, hidden), jnp.bfloat16)
    cuts = pl.pallas_call(
        functools.partial(cut_kernel, slots, hidden),
        out_shape=(jax.ShapeDtypeStruct((2 * block, hidden), jnp.bfloat16),) * (slots - 1)
        + (piece_shape,) * 2,
        in_specs=[smem] + [pl.BlockSpec(memory_space=pltpu.HBM)] * 2,
        out_specs=tuple(vmem_specs(slots + 1)),
        scratch_shapes=[pltpu.SemaphoreType.DMA((2 * slots,))],
        cost_estimate=pl.CostEstimate(flops=10**8, bytes_accessed=10**6, transcendentals=0),
        name="cut",
    )(index, up_weight, down_weight)
    early, middle, distant, last_ups, last_downs = cuts
    got = [along(packed[k], k) for k in range(slots)]
    keyval = jnp.stack([piece[:, :384] for piece in got])
    kv_pieces = [across(keyval, p) for p in range(plane - 1)]
    halves = (kv_pieces[2][: slots // 2], kv_pieces[1][slots // 2 :])
    kv_pieces.append(across(halves[0], 1))
    kv_pieces.append(across(halves[1], 2))

    firsts = [across(early, p) for p in range(3)]
    last_up = across(firsts[2][:block], 1)
    last_down = across(firsts[1][block:], 2)

    def gather(arrays):
        mine = jnp.concatenate(arrays, axis=0) if len(arrays) > 1 else arrays[0]
        near = [mine, across(mine, 1), across(mine, 2)]
        blocks = mine.shape[0] // block
        pieces = [
            [(p, near[p], i * block, 0, block) for p in range(3)] for i in range(blocks)
        ]
        split = mine.shape[0] // 2
        rows = math.gcd(block, split)
        for way, low in ((1, 0), (2, split)):
            sent = near[3 - way][low : low + split]
            far = across(sent, way)
            for row in range(low, low + split, rows):
                pieces[row // block].append((3, far, row - low, row % block, rows))
        return pieces

    def arrange(pieces):
        arrays = []
        moves = []
        for p, k, array, *rest in pieces:
            numbers = [i for i, other in enumerate(arrays) if other is array]
            if not numbers:
                numbers = [len(arrays)]
                arrays.append(array)
            moves.append((p, k, numbers[0], *rest))
        return pl.pallas_call(
            functools.partial(arrange_kernel, tuple(moves), plane, block),
            out_shape=jax.ShapeDtypeStruct((count * block, hidden), jnp.bfloat16),
            in_specs=[smem] + vmem_specs(len(arrays)),
            out_specs=pl.BlockSpec(memory_space=VMEM),
            compiler_params=pltpu.CompilerParams(vmem_limit_bytes=16 * 2**20),
            cost_estimate=pl.CostEstimate(flops=10**8, bytes_accessed=10**6, transcendentals=0),
        )(index, *arrays)

    own_up = [(p, 0, firsts[p], 0, 0, block) for p in range(3)]
    own_up.append((3, 0, last_up, 0, 0, block))
    own_down = [(p, 0, firsts[p], block, 0, block) for p in range(3)]
    own_down.append((3, 0, last_down, 0, 0, block))

    def label(k, pieces):
        return [(p, k, *rest) for p, *rest in pieces]

    first_moved = [along(middle, 1), along(last_ups, 3)]
    group = gather(first_moved)
    own_up += label(1, group[0]) + label(3, group[2])
    own_down += label(1, group[1])
    group = gather([along(distant, 2)])
    own_up += label(2, group[0])
    own_down += label(2, group[1])
    own_down += label(3, gather([along(last_downs, 3)])[0])
    up = arrange(own_up)
    down = arrange(own_down)

    sequence = count * tokens
    heads = pl.pallas_call(
        functools.partial(attend_kernel, slots, plane, tokens),
        out_shape=(jax.ShapeDtypeStruct((tokens, 192), jnp.bfloat16),) * slots,
        in_specs=[smem] * 3 + vmem_specs(3 + slots + plane),
        out_specs=tuple(vmem_specs(slots)),
        compiler_params=pltpu.CompilerParams(vmem_limit_bytes=24 * 2**20),
                scratch_shapes=[
            VMEM((slots, tokens, 192), jnp.bfloat16),
            VMEM((sequence, 384), jnp.bfloat16),
            VMEM((2 * tokens, sequence), jnp.float32),
            VMEM((slots, tokens, 192), jnp.bfloat16),
        ],
        cost_estimate=pl.CostEstimate(flops=8 * 10**9, bytes_accessed=2 * 10**6, transcendentals=0),
        name="attend",
    )(
        index,
        balance_first,
        balance_second,
        head_gain_first[None],
        head_gain_second[None],
        *got,
        *kv_pieces,
    )
    pieces = [along(heads[k], k) for k in range(slots)]
    row_shape = jax.ShapeDtypeStruct((half, width), jnp.bfloat16)
    own, other = pl.pallas_call(
        functools.partial(project_kernel, slots, half),
        out_shape=(row_shape, row_shape),
        in_specs=[smem] + vmem_specs(slots + 2),
        out_specs=tuple(vmem_specs(2)),
        scratch_shapes=[VMEM((slots, tokens, 192), jnp.bfloat16)],
        compiler_params=pltpu.CompilerParams(vmem_limit_bytes=16 * 2**20),
                cost_estimate=pl.CostEstimate(flops=2 * 10**9, bytes_accessed=4 * 10**6, transcendentals=0),
        name="project",
    )(index, *pieces, out_first, out_second)
    mixed, normed = pl.pallas_call(
        functools.partial(norm_kernel, half),
        out_shape=(row_shape, row_shape),
        in_specs=[smem] + vmem_specs(4),
        out_specs=tuple(vmem_specs(2)),
        compiler_params=pltpu.CompilerParams(vmem_limit_bytes=8 * 2**20),
                cost_estimate=pl.CostEstimate(flops=10**9, bytes_accessed=10**6, transcendentals=0),
        name="norm",
    )(index, residual, own, swap(other), mlp_gain[None])
    own_rows = [along(normed, k) for k in range(3)]
    own_rows.append(along(own_rows[2], 1))
    other_rows = [swap(piece) for piece in own_rows]
    group = slots // 2
    part_shape = jax.ShapeDtypeStruct((group, half, width), jnp.bfloat16)
    total = None

    def lift(chosen_slots):
        chosen = [own_rows[k] for k in chosen_slots] + [other_rows[k] for k in chosen_slots]
        return pl.pallas_call(
            lift_kernel,
            out_shape=jax.ShapeDtypeStruct((2 * group * half, hidden), jnp.bfloat16),
            in_specs=vmem_specs(1 + 2 * group),
            out_specs=pl.BlockSpec(memory_space=VMEM),
            scratch_shapes=[VMEM((2 * group * half, width), jnp.bfloat16)],
            compiler_params=pltpu.CompilerParams(vmem_limit_bytes=16 * 2**20),
            cost_estimate=pl.CostEstimate(flops=3 * 10**9, bytes_accessed=10**6, transcendentals=0),
        )(up, *chosen)

    def lower(active):
        return pl.pallas_call(
            lower_kernel,
            out_shape=(part_shape, part_shape),
            in_specs=vmem_specs(2),
            out_specs=tuple(vmem_specs(2)),
            compiler_params=pltpu.CompilerParams(vmem_limit_bytes=16 * 2**20),
            cost_estimate=pl.CostEstimate(flops=3 * 10**9, bytes_accessed=10**6, transcendentals=0),
        )(active, down)

    def finish(chosen):
        own, other = lower(lift(chosen))
        other = swap(other)
        summed = own.astype(jnp.float32) + other.astype(jnp.float32)
        return summed[0], summed[1]

    farthest, far = finish((3, 2))
    direct = 128 * round(width * DIRECT / 128)
    sent, far_sent = farthest.astype(jnp.bfloat16), far.astype(jnp.bfloat16)
    passed = along(sent[:, direct:], 1).astype(jnp.float32)
    straight = along(sent[:, :direct], 3).astype(jnp.float32)
    straight = straight + along(far_sent[:, :direct], 2).astype(jnp.float32)
    relayed = along((far[:, direct:] + passed).astype(jnp.bfloat16), 2).astype(jnp.float32)
    near, total = finish((1, 0))
    total = total + along(near.astype(jnp.bfloat16), 1).astype(jnp.float32)
    total = total + jnp.concatenate([straight, relayed], axis=1)
    mine = (mixed.astype(jnp.float32) + total).astype(jnp.bfloat16)
    theirs = swap(mine)
    return jnp.where(
        core == 0, jnp.concatenate([mine, theirs]), jnp.concatenate([theirs, mine])
    )


def dispatch(count, cores, *arguments):
    heads, other_heads = arguments[1].shape[1], arguments[4].shape[1]
    plane = count // heads
    fits = (
        cores == 2
        and heads == other_heads
        and plane == 4
        and heads == 4
        and plane * heads == count
        and arguments[3].shape[2] == 128
        and arguments[6].shape[2] == 64
    )
    if fits:
        return fast_body(heads, plane, *arguments)
    return body(*arguments)


def plan(mesh):
    return functools.partial(dispatch, mesh.shape["sp"], mesh.shape["tp"])


def solution(mesh):
    in_specs = (
        P("sp", None),
        P("sp", "tp", None),
        P("sp", "tp", None),
        P("sp", "tp", None),
        P("sp", "tp", None),
        P("sp", "tp", None),
        P("sp", "tp", None),
        P("tp"),
        P("tp"),
        P(),
        P(),
        P("tp", None),
        P("tp", None),
        P(),
        P("sp", "tp"),
        P("sp", "tp"),
    )
    out_specs = P("sp", None)
    return jax.shard_map(
        plan(mesh), mesh=mesh, in_specs=in_specs, out_specs=out_specs, check_vma=False
    )
```

```python
import functools
import math

import jax
import jax.numpy as jnp
from jax import lax
from jax.experimental import pallas as pl
from jax.experimental.pallas import tpu as pltpu
from jax.sharding import PartitionSpec as P

DK_A = 64
DK_B = 32


EPSILON = 1e-06
HEAD_SCALE = 0.8


def attend(queries, keys, values, balance, gain, device, head_size):
    tokens = queries.shape[0]
    heads = queries.shape[1]
    seq = keys.shape[0]
    depth = values.shape[2]
    block = math.gcd(512, seq)
    scale = head_size ** (-0.5)
    query_maps = queries.reshape(tokens, heads, 2, head_size)
    key_maps = keys.reshape(seq, heads, 2, head_size)
    first_row = device * tokens
    positions = first_row + jnp.arange(tokens, dtype=jnp.int32)
    needed = (first_row + tokens + block - 1) // block

    def block_scores(number):
        start = number * block
        key_block = lax.dynamic_slice_in_dim(key_maps, start, block, 0)
        scores = (
            jnp.einsum("qhmd,khmd->hmqk", query_maps, key_block, preferred_element_type=jnp.float32)
            * scale
        )
        columns = start + jnp.arange(block, dtype=jnp.int32)
        visible = columns[None, :] <= positions[:, None]
        return (jnp.where(visible, scores, -jnp.inf), start)

    def statistics(number, carry):
        highest, total = carry
        scores, _ = block_scores(number)
        fresh = jnp.maximum(highest, jnp.max(scores, axis=-1, keepdims=True))
        total = total * jnp.exp(highest - fresh) + jnp.sum(
            jnp.exp(scores - fresh), axis=-1, keepdims=True
        )
        return (fresh, total)

    start_high = jnp.full((heads, 2, tokens, 1), -jnp.inf, jnp.float32)
    start_total = jnp.zeros((heads, 2, tokens, 1), jnp.float32)
    highest, total = lax.fori_loop(0, needed, statistics, (start_high, start_total))

    def accumulate(number, result):
        scores, start = block_scores(number)
        probs = jnp.exp(scores - highest) / total
        mixed = (probs[:, 0] - balance[:, None, None] * probs[:, 1]).astype(jnp.bfloat16)
        value_block = lax.dynamic_slice_in_dim(values, start, block, 0)
        return result + jnp.einsum(
            "hqk,khe->qhe", mixed, value_block, preferred_element_type=jnp.float32
        )

    summed = lax.fori_loop(0, needed, accumulate, jnp.zeros((tokens, heads, depth), jnp.float32))
    power = jnp.mean(summed * summed, axis=-1, keepdims=True)
    normed = summed * lax.rsqrt(power + EPSILON) * gain * HEAD_SCALE
    return normed.astype(jnp.bfloat16).reshape(tokens, heads * depth)


def body(
    residual,
    query_first,
    key_first,
    value_first,
    query_second,
    key_second,
    value_second,
    balance_first,
    balance_second,
    head_gain_first,
    head_gain_second,
    out_first,
    out_second,
    mlp_gain,
    up_weight,
    down_weight,
):
    device = lax.axis_index("sp")
    keys_first, values_first, keys_second, values_second = (
        lax.all_gather(key_first, "sp", axis=0, tiled=True),
        lax.all_gather(value_first, "sp", axis=0, tiled=True),
        lax.all_gather(key_second, "sp", axis=0, tiled=True),
        lax.all_gather(value_second, "sp", axis=0, tiled=True),
    )
    heads_first = attend(
        query_first, keys_first, values_first, balance_first, head_gain_first, device, DK_A
    )
    heads_second = attend(
        query_second, keys_second, values_second, balance_second, head_gain_second, device, DK_B
    )
    head_term = jnp.dot(heads_first, out_first, preferred_element_type=jnp.float32) + jnp.dot(
        heads_second, out_second, preferred_element_type=jnp.float32
    )
    head_total = lax.psum(head_term.astype(jnp.bfloat16), "tp").astype(jnp.float32)
    mixed = (residual.astype(jnp.float32) + head_total).astype(jnp.bfloat16)
    mixed_float = mixed.astype(jnp.float32)
    power = jnp.mean(mixed_float * mixed_float, axis=-1, keepdims=True)
    normed = (mixed_float * lax.rsqrt(power + EPSILON) * mlp_gain).astype(jnp.bfloat16)
    up_whole, down_whole = (
        lax.all_gather(up_weight, "sp", axis=0, tiled=True),
        lax.all_gather(down_weight, "sp", axis=0, tiled=True),
    )
    lifted = jnp.dot(normed, up_whole, preferred_element_type=jnp.float32)
    active = jax.nn.relu(lifted)
    hidden = (active * active).astype(jnp.bfloat16)
    down_term = lax.dot_general(
        hidden, down_whole, (((1,), (1,)), ((), ())), preferred_element_type=jnp.float32
    )
    added = lax.psum(down_term.astype(jnp.bfloat16), "tp").astype(jnp.float32)
    return (mixed_float + added).astype(jnp.bfloat16)


VMEM = pltpu.VMEM
SMEM = pltpu.SMEM
DIRECT = 0.25


def vmem_specs(count):
    return [pl.BlockSpec(memory_space=VMEM)] * count


def pack_kernel(slots, plane, *refs):
    sources, outs, held = refs[:6], refs[6 : 6 + slots], refs[6 + slots : -2]
    packed, arrived = refs[-2:]
    z = lax.axis_index("sp") // plane
    copies = [
        pltpu.make_async_copy(source, target, arrived.at[i])
        for i, (source, target) in enumerate(zip(sources, held))
    ]
    for copy in copies:
        copy.start()
    for copy in copies:
        copy.wait()
    key_a, key_b, value_b, value_a, query_a, query_b = held
    for head in range(slots):
        packed[head, :, 0:128] = key_a[:, head, :]
        packed[head, :, 128:192] = key_b[head].T
        packed[head, :, 192:256] = value_b[head].T
        packed[head, :, 256:384] = value_a[:, head, :]
        packed[head, :, 384:512] = query_a[:, head, :]
        packed[head, :, 512:576] = query_b[head].T
    for k in range(slots):
        outs[k][...] = packed[z ^ k]


def cut_kernel(slots, plane, width, *refs):
    weights, pairs, lasts = refs[:2], refs[2 : 1 + slots], refs[1 + slots : -1]
    arrived = refs[-1]
    z = lax.axis_index("sp") // plane
    block = weights[0].shape[0]
    copies = []
    for i, (weight, last) in enumerate(zip(weights, lasts)):
        for k in range(slots):
            place = pl.ds(pl.multiple_of((z ^ k) * width, width), width)
            target = last if k == slots - 1 else pairs[k].at[pl.ds(i * block, block), :]
            copies.append(
                pltpu.make_async_copy(weight.at[:, place], target, arrived.at[i * slots + k])
            )
    for copy in copies:
        copy.start()
    for copy in copies:
        copy.wait()


def attend_kernel(slots, plane, tokens, index, balance_a, balance_b, gain_a, gain_b, *refs):
    queries, kv_pieces = refs[:slots], refs[slots : slots + plane + 1]
    outs = refs[slots + plane + 1 : 2 * slots + plane + 1]
    query, keyval, scores, out = refs[2 * slots + plane + 1 :]
    z, g = index[0], index[1]
    wide = plane * tokens
    for k in range(slots):
        query[z ^ k] = queries[k][:, 384:576]
        for p in range(plane):
            start = pl.multiple_of(((z ^ k) * plane + (g ^ p)) * tokens, tokens)
            if p < plane - 1:
                keyval[pl.ds(start, tokens), :] = kv_pieces[p][k]
            else:
                part = slots // 2
                keyval[pl.ds(start, tokens), :] = kv_pieces[p + k // part][k % part]
    lane = lax.broadcasted_iota(jnp.int32, (tokens, 128), 1)
    row = lax.broadcasted_iota(jnp.int32, (2 * tokens, wide), 0) % tokens
    column = lax.broadcasted_iota(jnp.int32, (2 * tokens, wide), 1)
    visible = column <= row + g * tokens

    def group(number, place, size, key_lo, value_lo, balance):
        packed = query[number][:, place : place + 2 * size]
        if 2 * size < 128:
            packed = jnp.concatenate(
                [packed, jnp.zeros((tokens, 128 - 2 * size), packed.dtype)], axis=1
            )
        zero = jnp.zeros_like(packed)
        both = jnp.concatenate(
            [jnp.where(lane < size, packed, zero), jnp.where(lane >= size, packed, zero)], axis=0
        )
        factor = size ** (-0.5) * math.log2(math.e)
        highest = None
        for c in range(number + 1):
            part = lax.dot_general(
                both,
                keyval[c * wide : (c + 1) * wide, key_lo : key_lo + 128],
                (((1,), (1,)), ((), ())),
                preferred_element_type=jnp.float32,
            )
            if c == number:
                part = jnp.where(visible, part, -jnp.inf)
            scores[:, c * wide : (c + 1) * wide] = part
            top = jnp.max(part, axis=1, keepdims=True)
            highest = top if highest is None else jnp.maximum(highest, top)
        total = jnp.zeros((2 * tokens, 1), jnp.float32)
        for c in range(number + 1):
            part = jnp.exp2((scores[:, c * wide : (c + 1) * wide] - highest) * factor)
            scores[:, c * wide : (c + 1) * wide] = part
            total = total + jnp.sum(part, axis=1, keepdims=True)
        share = 1.0 / total
        first, second = share[:tokens], share[tokens:] * balance
        summed = jnp.zeros((tokens, 128), jnp.float32)
        for c in range(number + 1):
            span = slice(c * wide, (c + 1) * wide)
            weights = (scores[:tokens, span] * first - scores[tokens:, span] * second).astype(
                jnp.bfloat16
            )
            summed = summed + jnp.dot(
                weights, keyval[span, value_lo : value_lo + 128], preferred_element_type=jnp.float32
            )
        return summed

    def normed(summed, gain):
        power = jnp.mean(summed * summed, axis=-1, keepdims=True)
        return (summed * lax.rsqrt(power + EPSILON) * gain[...] * HEAD_SCALE).astype(jnp.bfloat16)

    for number in range(slots):
        summed = group(number, 0, DK_A, 0, 256, balance_a[z])
        out[number, :, 0:128] = normed(summed, gain_a)
        summed = group(number, 128, DK_B, 128, 128, balance_b[z])[:, 64:128]
        out[number, :, 128:192] = normed(summed, gain_b)
    for k in range(slots):
        outs[k][...] = out[z ^ k]


def project_kernel(slots, half, index, *refs):
    pieces, out_a, out_b, own, other, left = (
        refs[:slots],
        refs[slots],
        refs[slots + 1],
        refs[slots + 2],
        refs[slots + 3],
        refs[slots + 4],
    )
    z, core = index[0], index[2]
    mine = pl.multiple_of(core * half, half)
    theirs = pl.multiple_of((1 - core) * half, half)
    for k in range(slots):
        left[k, :half] = pieces[k][pl.ds(mine, half), :]
        left[k, half:] = pieces[k][pl.ds(theirs, half), :]
    tile = 512
    for n in range(out_a.shape[1] // tile):
        span = slice(n * tile, (n + 1) * tile)
        total = jnp.zeros((2 * half, tile), jnp.float32)
        for k in range(slots):
            head = z ^ k
            total += jnp.dot(
                left[k, :, 0:128],
                out_a[pl.ds(pl.multiple_of(head * 128, 128), 128), span],
                preferred_element_type=jnp.float32,
            )
            total += jnp.dot(
                left[k, :, 128:192],
                out_b[pl.ds(pl.multiple_of(head * 64, 64), 64), span],
                preferred_element_type=jnp.float32,
            )
        total = total.astype(jnp.bfloat16)
        own[:, span] = total[:half]
        other[:, span] = total[half:]


def norm_kernel(half, index, residual, own, other, gain, mixed, normed):
    mine = pl.multiple_of(index[2] * half, half)
    total = own[...].astype(jnp.float32) + other[...].astype(jnp.float32)
    rounded = (residual[pl.ds(mine, half), :].astype(jnp.float32) + total).astype(jnp.bfloat16)
    mixed[...] = rounded
    value = rounded.astype(jnp.float32)
    power = jnp.mean(value * value, axis=-1, keepdims=True)
    normed[...] = (value * lax.rsqrt(power + EPSILON) * gain[...]).astype(jnp.bfloat16)


def arrange_kernel(moves, plane, block, index, *refs):
    out = refs[-1]
    z, g = index[0], index[1]
    for p, k, number, source, target, rows in moves:
        place = ((z ^ k) * plane + (g ^ p)) * block + target
        out[pl.ds(pl.multiple_of(place, rows), rows), :] = refs[number][source : source + rows, :]


def lift_kernel(up, *refs):
    rows, hidden, left = refs[:-2], refs[-2], refs[-1]
    half = rows[0].shape[0]
    for r, piece in enumerate(rows):
        left[r * half : (r + 1) * half, :] = piece[...]
    tile = 256
    for n in range(up.shape[1] // tile):
        span = slice(n * tile, (n + 1) * tile)
        active = jnp.maximum(
            jnp.dot(left[...], up[:, span], preferred_element_type=jnp.float32), 0.0
        )
        hidden[:, span] = (active * active).astype(jnp.bfloat16)


def lower_kernel(hidden, down, own, other):
    count, half, width = own.shape
    tile = 512
    for n in range(width // tile):
        span = slice(n * tile, (n + 1) * tile)
        part = lax.dot_general(
            hidden[...],
            down[span, :],
            (((1,), (1,)), ((), ())),
            preferred_element_type=jnp.float32,
        ).astype(jnp.bfloat16)
        for r in range(count):
            rest = (r + count) * half
            own[r, :, span] = part[r * half : (r + 1) * half]
            other[r, :, span] = part[rest : rest + half]


def fast_body(slots, plane, *arguments):
    (
        residual,
        query_first,
        key_first,
        value_first,
        query_second,
        key_second,
        value_second,
        balance_first,
        balance_second,
        head_gain_first,
        head_gain_second,
        out_first,
        out_second,
        mlp_gain,
        up_weight,
        down_weight,
    ) = arguments
    count = slots * plane
    tokens, width = residual.shape
    half = tokens // 2
    device, core = lax.axis_index("sp"), lax.axis_index("tp")
    z, g = device // plane, device % plane
    index = jnp.stack([z, g, core]).astype(jnp.int32)

    def along(value, k):
        if k == 0:
            return value
        return lax.ppermute(
            value, "sp", [(i, (i // plane ^ k) * plane + i % plane) for i in range(count)]
        )

    def across(value, k):
        if k == 0:
            return value
        return lax.ppermute(value, "sp", [(i, i ^ k) for i in range(count)])

    def swap(value):
        return lax.ppermute(value, "tp", [(0, 1), (1, 0)])

    smem = pl.BlockSpec(memory_space=SMEM)
    hidden = up_weight.shape[1] // slots
    block = up_weight.shape[0]
    sources = (
        key_first,
        key_second.transpose(1, 2, 0),
        value_second.transpose(1, 2, 0),
        value_first,
        query_first,
        query_second.transpose(1, 2, 0),
    )
    packed = pl.pallas_call(
        functools.partial(pack_kernel, slots, plane),
        out_shape=(jax.ShapeDtypeStruct((tokens, 576), jnp.bfloat16),) * slots,
        in_specs=[pl.BlockSpec(memory_space=pltpu.HBM)] * 6,
        out_specs=tuple(vmem_specs(slots)),
        scratch_shapes=[VMEM(source.shape, jnp.bfloat16) for source in sources]
        + [VMEM((slots, tokens, 576), jnp.bfloat16), pltpu.SemaphoreType.DMA((6,))],
        cost_estimate=pl.CostEstimate(flops=10**8, bytes_accessed=10**6, transcendentals=0),
        name="pack",
    )(*sources)
    piece_shape = jax.ShapeDtypeStruct((block, hidden), jnp.bfloat16)
    cuts = pl.pallas_call(
        functools.partial(cut_kernel, slots, plane, hidden),
        out_shape=(jax.ShapeDtypeStruct((2 * block, hidden), jnp.bfloat16),) * (slots - 1)
        + (piece_shape,) * 2,
        in_specs=[pl.BlockSpec(memory_space=pltpu.HBM)] * 2,
        out_specs=tuple(vmem_specs(slots + 1)),
        scratch_shapes=[pltpu.SemaphoreType.DMA((2 * slots,))],
        cost_estimate=pl.CostEstimate(flops=10**8, bytes_accessed=10**6, transcendentals=0),
        name="cut",
    )(up_weight, down_weight)
    early, middle, distant, last_ups, last_downs = cuts
    got = [along(packed[k], k) for k in range(slots)]
    keyval = jnp.stack([piece[:, :384] for piece in got])
    kv_pieces = [across(keyval, p) for p in range(plane - 1)]
    halves = (kv_pieces[2][: slots // 2], kv_pieces[1][slots // 2 :])
    kv_pieces.append(across(halves[0], 1))
    kv_pieces.append(across(halves[1], 2))

    firsts = [across(early, p) for p in range(3)]
    last_up = across(firsts[2][:block], 1)
    last_down = across(firsts[1][block:], 2)

    def gather(arrays):
        mine = jnp.concatenate(arrays, axis=0) if len(arrays) > 1 else arrays[0]
        near = [mine, across(mine, 1), across(mine, 2)]
        blocks = mine.shape[0] // block
        pieces = [
            [(p, near[p], i * block, 0, block) for p in range(3)] for i in range(blocks)
        ]
        split = mine.shape[0] // 2
        rows = math.gcd(block, split)
        for way, low in ((1, 0), (2, split)):
            sent = near[3 - way][low : low + split]
            far = across(sent, way)
            for row in range(low, low + split, rows):
                pieces[row // block].append((3, far, row - low, row % block, rows))
        return pieces

    def arrange(pieces):
        arrays = []
        moves = []
        for p, k, array, *rest in pieces:
            numbers = [i for i, other in enumerate(arrays) if other is array]
            if not numbers:
                numbers = [len(arrays)]
                arrays.append(array)
            moves.append((p, k, numbers[0], *rest))
        return pl.pallas_call(
            functools.partial(arrange_kernel, tuple(moves), plane, block),
            out_shape=jax.ShapeDtypeStruct((count * block, hidden), jnp.bfloat16),
            in_specs=[smem] + vmem_specs(len(arrays)),
            out_specs=pl.BlockSpec(memory_space=VMEM),
            compiler_params=pltpu.CompilerParams(vmem_limit_bytes=16 * 2**20),
            cost_estimate=pl.CostEstimate(flops=10**8, bytes_accessed=10**6, transcendentals=0),
        )(index, *arrays)

    own_up = [(p, 0, firsts[p], 0, 0, block) for p in range(3)]
    own_up.append((3, 0, last_up, 0, 0, block))
    own_down = [(p, 0, firsts[p], block, 0, block) for p in range(3)]
    own_down.append((3, 0, last_down, 0, 0, block))

    def label(k, pieces):
        return [(p, k, *rest) for p, *rest in pieces]

    first_moved = [along(middle, 1), along(last_ups, 3)]
    group = gather(first_moved)
    own_up += label(1, group[0]) + label(3, group[2])
    own_down += label(1, group[1])
    group = gather([along(distant, 2)])
    own_up += label(2, group[0])
    own_down += label(2, group[1])
    own_down += label(3, gather([along(last_downs, 3)])[0])
    up = arrange(own_up)
    down = arrange(own_down)

    sequence = count * tokens
    heads = pl.pallas_call(
        functools.partial(attend_kernel, slots, plane, tokens),
        out_shape=(jax.ShapeDtypeStruct((tokens, 192), jnp.bfloat16),) * slots,
        in_specs=[smem] * 3 + vmem_specs(3 + slots + plane),
        out_specs=tuple(vmem_specs(slots)),
        compiler_params=pltpu.CompilerParams(vmem_limit_bytes=24 * 2**20),
                scratch_shapes=[
            VMEM((slots, tokens, 192), jnp.bfloat16),
            VMEM((sequence, 384), jnp.bfloat16),
            VMEM((2 * tokens, sequence), jnp.float32),
            VMEM((slots, tokens, 192), jnp.bfloat16),
        ],
        cost_estimate=pl.CostEstimate(flops=8 * 10**9, bytes_accessed=2 * 10**6, transcendentals=0),
        name="attend",
    )(
        index,
        balance_first,
        balance_second,
        head_gain_first[None],
        head_gain_second[None],
        *got,
        *kv_pieces,
    )
    pieces = [along(heads[k], k) for k in range(slots)]
    row_shape = jax.ShapeDtypeStruct((half, width), jnp.bfloat16)
    own, other = pl.pallas_call(
        functools.partial(project_kernel, slots, half),
        out_shape=(row_shape, row_shape),
        in_specs=[smem] + vmem_specs(slots + 2),
        out_specs=tuple(vmem_specs(2)),
        scratch_shapes=[VMEM((slots, tokens, 192), jnp.bfloat16)],
        compiler_params=pltpu.CompilerParams(vmem_limit_bytes=16 * 2**20),
                cost_estimate=pl.CostEstimate(flops=2 * 10**9, bytes_accessed=4 * 10**6, transcendentals=0),
        name="project",
    )(index, *pieces, out_first, out_second)
    mixed, normed = pl.pallas_call(
        functools.partial(norm_kernel, half),
        out_shape=(row_shape, row_shape),
        in_specs=[smem] + vmem_specs(4),
        out_specs=tuple(vmem_specs(2)),
        compiler_params=pltpu.CompilerParams(vmem_limit_bytes=8 * 2**20),
                cost_estimate=pl.CostEstimate(flops=10**9, bytes_accessed=10**6, transcendentals=0),
        name="norm",
    )(index, residual, own, swap(other), mlp_gain[None])
    own_rows = [along(normed, k) for k in range(3)]
    own_rows.append(along(own_rows[2], 1))
    other_rows = [swap(piece) for piece in own_rows]
    group = slots // 2
    part_shape = jax.ShapeDtypeStruct((group, half, width), jnp.bfloat16)
    total = None

    def lift(chosen_slots):
        chosen = [own_rows[k] for k in chosen_slots] + [other_rows[k] for k in chosen_slots]
        return pl.pallas_call(
            lift_kernel,
            out_shape=jax.ShapeDtypeStruct((2 * group * half, hidden), jnp.bfloat16),
            in_specs=vmem_specs(1 + 2 * group),
            out_specs=pl.BlockSpec(memory_space=VMEM),
            scratch_shapes=[VMEM((2 * group * half, width), jnp.bfloat16)],
            compiler_params=pltpu.CompilerParams(vmem_limit_bytes=16 * 2**20),
            cost_estimate=pl.CostEstimate(flops=3 * 10**9, bytes_accessed=10**6, transcendentals=0),
        )(up, *chosen)

    def lower(active):
        return pl.pallas_call(
            lower_kernel,
            out_shape=(part_shape, part_shape),
            in_specs=vmem_specs(2),
            out_specs=tuple(vmem_specs(2)),
            compiler_params=pltpu.CompilerParams(vmem_limit_bytes=16 * 2**20),
            cost_estimate=pl.CostEstimate(flops=3 * 10**9, bytes_accessed=10**6, transcendentals=0),
        )(active, down)

    def finish(chosen):
        own, other = lower(lift(chosen))
        other = swap(other)
        summed = own.astype(jnp.float32) + other.astype(jnp.float32)
        return summed[0], summed[1]

    farthest, far = finish((3, 2))
    direct = 128 * round(width * DIRECT / 128)
    sent, far_sent = farthest.astype(jnp.bfloat16), far.astype(jnp.bfloat16)
    passed = along(sent[:, direct:], 1).astype(jnp.float32)
    straight = along(sent[:, :direct], 3).astype(jnp.float32)
    straight = straight + along(far_sent[:, :direct], 2).astype(jnp.float32)
    relayed = along((far[:, direct:] + passed).astype(jnp.bfloat16), 2).astype(jnp.float32)
    near, total = finish((1, 0))
    total = total + along(near.astype(jnp.bfloat16), 1).astype(jnp.float32)
    total = total + jnp.concatenate([straight, relayed], axis=1)
    mine = (mixed.astype(jnp.float32) + total).astype(jnp.bfloat16)
    theirs = swap(mine)
    return jnp.where(
        core == 0, jnp.concatenate([mine, theirs]), jnp.concatenate([theirs, mine])
    )


def dispatch(count, cores, *arguments):
    heads, other_heads = arguments[1].shape[1], arguments[4].shape[1]
    plane = count // heads
    fits = (
        cores == 2
        and heads == other_heads
        and plane == 4
        and heads == 4
        and plane * heads == count
        and arguments[3].shape[2] == 128
        and arguments[6].shape[2] == 64
    )
    if fits:
        return fast_body(heads, plane, *arguments)
    return body(*arguments)


def plan(mesh):
    return functools.partial(dispatch, mesh.shape["sp"], mesh.shape["tp"])


def solution(mesh):
    in_specs = (
        P("sp", None),
        P("sp", "tp", None),
        P("sp", "tp", None),
        P("sp", "tp", None),
        P("sp", "tp", None),
        P("sp", "tp", None),
        P("sp", "tp", None),
        P("tp"),
        P("tp"),
        P(),
        P(),
        P("tp", None),
        P("tp", None),
        P(),
        P("sp", "tp"),
        P("sp", "tp"),
    )
    out_specs = P("sp", None)
    return jax.shard_map(
        plan(mesh), mesh=mesh, in_specs=in_specs, out_specs=out_specs, check_vma=False
    )
```

```python
import functools
import math

import jax
import jax.numpy as jnp
from jax import lax
from jax.experimental import pallas as pl
from jax.experimental.pallas import tpu as pltpu
from jax.sharding import PartitionSpec as P

DK_A = 64
DK_B = 32


EPSILON = 1e-06
HEAD_SCALE = 0.8


def attend(queries, keys, values, balance, gain, device, head_size):
    tokens = queries.shape[0]
    heads = queries.shape[1]
    seq = keys.shape[0]
    depth = values.shape[2]
    block = math.gcd(512, seq)
    scale = head_size ** (-0.5)
    query_maps = queries.reshape(tokens, heads, 2, head_size)
    key_maps = keys.reshape(seq, heads, 2, head_size)
    first_row = device * tokens
    positions = first_row + jnp.arange(tokens, dtype=jnp.int32)
    needed = (first_row + tokens + block - 1) // block

    def block_scores(number):
        start = number * block
        key_block = lax.dynamic_slice_in_dim(key_maps, start, block, 0)
        scores = (
            jnp.einsum("qhmd,khmd->hmqk", query_maps, key_block, preferred_element_type=jnp.float32)
            * scale
        )
        columns = start + jnp.arange(block, dtype=jnp.int32)
        visible = columns[None, :] <= positions[:, None]
        return (jnp.where(visible, scores, -jnp.inf), start)

    def statistics(number, carry):
        highest, total = carry
        scores, _ = block_scores(number)
        fresh = jnp.maximum(highest, jnp.max(scores, axis=-1, keepdims=True))
        total = total * jnp.exp(highest - fresh) + jnp.sum(
            jnp.exp(scores - fresh), axis=-1, keepdims=True
        )
        return (fresh, total)

    start_high = jnp.full((heads, 2, tokens, 1), -jnp.inf, jnp.float32)
    start_total = jnp.zeros((heads, 2, tokens, 1), jnp.float32)
    highest, total = lax.fori_loop(0, needed, statistics, (start_high, start_total))

    def accumulate(number, result):
        scores, start = block_scores(number)
        probs = jnp.exp(scores - highest) / total
        mixed = (probs[:, 0] - balance[:, None, None] * probs[:, 1]).astype(jnp.bfloat16)
        value_block = lax.dynamic_slice_in_dim(values, start, block, 0)
        return result + jnp.einsum(
            "hqk,khe->qhe", mixed, value_block, preferred_element_type=jnp.float32
        )

    summed = lax.fori_loop(0, needed, accumulate, jnp.zeros((tokens, heads, depth), jnp.float32))
    power = jnp.mean(summed * summed, axis=-1, keepdims=True)
    normed = summed * lax.rsqrt(power + EPSILON) * gain * HEAD_SCALE
    return normed.astype(jnp.bfloat16).reshape(tokens, heads * depth)


def body(
    residual,
    query_first,
    key_first,
    value_first,
    query_second,
    key_second,
    value_second,
    balance_first,
    balance_second,
    head_gain_first,
    head_gain_second,
    out_first,
    out_second,
    mlp_gain,
    up_weight,
    down_weight,
):
    device = lax.axis_index("sp")
    keys_first, values_first, keys_second, values_second = (
        lax.all_gather(key_first, "sp", axis=0, tiled=True),
        lax.all_gather(value_first, "sp", axis=0, tiled=True),
        lax.all_gather(key_second, "sp", axis=0, tiled=True),
        lax.all_gather(value_second, "sp", axis=0, tiled=True),
    )
    heads_first = attend(
        query_first, keys_first, values_first, balance_first, head_gain_first, device, DK_A
    )
    heads_second = attend(
        query_second, keys_second, values_second, balance_second, head_gain_second, device, DK_B
    )
    head_term = jnp.dot(heads_first, out_first, preferred_element_type=jnp.float32) + jnp.dot(
        heads_second, out_second, preferred_element_type=jnp.float32
    )
    head_total = lax.psum(head_term.astype(jnp.bfloat16), "tp").astype(jnp.float32)
    mixed = (residual.astype(jnp.float32) + head_total).astype(jnp.bfloat16)
    mixed_float = mixed.astype(jnp.float32)
    power = jnp.mean(mixed_float * mixed_float, axis=-1, keepdims=True)
    normed = (mixed_float * lax.rsqrt(power + EPSILON) * mlp_gain).astype(jnp.bfloat16)
    up_whole, down_whole = (
        lax.all_gather(up_weight, "sp", axis=0, tiled=True),
        lax.all_gather(down_weight, "sp", axis=0, tiled=True),
    )
    lifted = jnp.dot(normed, up_whole, preferred_element_type=jnp.float32)
    active = jax.nn.relu(lifted)
    hidden = (active * active).astype(jnp.bfloat16)
    down_term = lax.dot_general(
        hidden, down_whole, (((1,), (1,)), ((), ())), preferred_element_type=jnp.float32
    )
    added = lax.psum(down_term.astype(jnp.bfloat16), "tp").astype(jnp.float32)
    return (mixed_float + added).astype(jnp.bfloat16)


VMEM = pltpu.VMEM
SMEM = pltpu.SMEM
DIRECT = 0.25


def vmem_specs(count):
    return [pl.BlockSpec(memory_space=VMEM)] * count


def pack_kernel(slots, plane, *refs):
    sources, outs, held = refs[:6], refs[6 : 6 + slots], refs[6 + slots : -2]
    packed, arrived = refs[-2:]
    z = lax.axis_index("sp") // plane
    copies = [
        pltpu.make_async_copy(source, target, arrived.at[i])
        for i, (source, target) in enumerate(zip(sources, held))
    ]
    for copy in copies:
        copy.start()
    for copy in copies:
        copy.wait()
    key_a, key_b, value_b, value_a, query_a, query_b = held
    for head in range(slots):
        packed[head, :, 0:128] = key_a[:, head, :]
        packed[head, :, 128:192] = key_b[head].T
        packed[head, :, 192:256] = value_b[head].T
        packed[head, :, 256:384] = value_a[:, head, :]
        packed[head, :, 384:512] = query_a[:, head, :]
        packed[head, :, 512:576] = query_b[head].T
    for k in range(slots):
        outs[k][...] = packed[z ^ k]


def cut_kernel(slots, plane, width, *refs):
    weights, pairs, lasts = refs[:2], refs[2 : 1 + slots], refs[1 + slots : -1]
    arrived = refs[-1]
    z = lax.axis_index("sp") // plane
    block = weights[0].shape[0]
    copies = []
    for i, (weight, last) in enumerate(zip(weights, lasts)):
        for k in range(slots):
            place = pl.ds(pl.multiple_of((z ^ k) * width, width), width)
            target = last if k == slots - 1 else pairs[k].at[pl.ds(i * block, block), :]
            copies.append(
                pltpu.make_async_copy(weight.at[:, place], target, arrived.at[i * slots + k])
            )
    for copy in copies:
        copy.start()
    for copy in copies:
        copy.wait()


def attend_kernel(slots, plane, tokens, index, balance_a, balance_b, gain_a, gain_b, *refs):
    queries, kv_pieces = refs[:slots], refs[slots : slots + plane + 1]
    outs = refs[slots + plane + 1 : 2 * slots + plane + 1]
    query, keyval, scores, out = refs[2 * slots + plane + 1 :]
    z, g = index[0], index[1]
    wide = plane * tokens
    for k in range(slots):
        query[z ^ k] = queries[k][:, 384:576]
        for p in range(plane):
            start = pl.multiple_of(((z ^ k) * plane + (g ^ p)) * tokens, tokens)
            if p < plane - 1:
                keyval[pl.ds(start, tokens), :] = kv_pieces[p][k]
            else:
                part = slots // 2
                keyval[pl.ds(start, tokens), :] = kv_pieces[p + k // part][k % part]
    lane = lax.broadcasted_iota(jnp.int32, (tokens, 128), 1)
    row = lax.broadcasted_iota(jnp.int32, (2 * tokens, wide), 0) % tokens
    column = lax.broadcasted_iota(jnp.int32, (2 * tokens, wide), 1)
    visible = column <= row + g * tokens

    def group(number, place, size, key_lo, value_lo, balance):
        packed = query[number][:, place : place + 2 * size]
        if 2 * size < 128:
            packed = jnp.concatenate(
                [packed, jnp.zeros((tokens, 128 - 2 * size), packed.dtype)], axis=1
            )
        zero = jnp.zeros_like(packed)
        both = jnp.concatenate(
            [jnp.where(lane < size, packed, zero), jnp.where(lane >= size, packed, zero)], axis=0
        )
        factor = size ** (-0.5) * math.log2(math.e)
        highest = None
        for c in range(number + 1):
            part = lax.dot_general(
                both,
                keyval[c * wide : (c + 1) * wide, key_lo : key_lo + 128],
                (((1,), (1,)), ((), ())),
                preferred_element_type=jnp.float32,
            )
            if c == number:
                part = jnp.where(visible, part, -jnp.inf)
            scores[:, c * wide : (c + 1) * wide] = part
            top = jnp.max(part, axis=1, keepdims=True)
            highest = top if highest is None else jnp.maximum(highest, top)
        total = jnp.zeros((2 * tokens, 1), jnp.float32)
        for c in range(number + 1):
            part = jnp.exp2((scores[:, c * wide : (c + 1) * wide] - highest) * factor)
            scores[:, c * wide : (c + 1) * wide] = part
            total = total + jnp.sum(part, axis=1, keepdims=True)
        share = 1.0 / total
        first, second = share[:tokens], share[tokens:] * balance
        summed = jnp.zeros((tokens, 128), jnp.float32)
        for c in range(number + 1):
            span = slice(c * wide, (c + 1) * wide)
            weights = (scores[:tokens, span] * first - scores[tokens:, span] * second).astype(
                jnp.bfloat16
            )
            summed = summed + jnp.dot(
                weights, keyval[span, value_lo : value_lo + 128], preferred_element_type=jnp.float32
            )
        return summed

    def normed(summed, gain):
        power = jnp.mean(summed * summed, axis=-1, keepdims=True)
        return (summed * lax.rsqrt(power + EPSILON) * gain[...] * HEAD_SCALE).astype(jnp.bfloat16)

    for number in range(slots):
        summed = group(number, 0, DK_A, 0, 256, balance_a[z])
        out[number, :, 0:128] = normed(summed, gain_a)
        summed = group(number, 128, DK_B, 128, 128, balance_b[z])[:, 64:128]
        out[number, :, 128:192] = normed(summed, gain_b)
    for k in range(slots):
        outs[k][...] = out[z ^ k]


def project_kernel(slots, half, index, *refs):
    pieces, out_a, out_b, own, other, left = (
        refs[:slots],
        refs[slots],
        refs[slots + 1],
        refs[slots + 2],
        refs[slots + 3],
        refs[slots + 4],
    )
    z, core = index[0], index[2]
    mine = pl.multiple_of(core * half, half)
    theirs = pl.multiple_of((1 - core) * half, half)
    for k in range(slots):
        left[k, :half] = pieces[k][pl.ds(mine, half), :]
        left[k, half:] = pieces[k][pl.ds(theirs, half), :]
    tile = 512
    for n in range(out_a.shape[1] // tile):
        span = slice(n * tile, (n + 1) * tile)
        total = jnp.zeros((2 * half, tile), jnp.float32)
        for k in range(slots):
            head = z ^ k
            total += jnp.dot(
                left[k, :, 0:128],
                out_a[pl.ds(pl.multiple_of(head * 128, 128), 128), span],
                preferred_element_type=jnp.float32,
            )
            total += jnp.dot(
                left[k, :, 128:192],
                out_b[pl.ds(pl.multiple_of(head * 64, 64), 64), span],
                preferred_element_type=jnp.float32,
            )
        total = total.astype(jnp.bfloat16)
        own[:, span] = total[:half]
        other[:, span] = total[half:]


def norm_kernel(half, index, residual, own, other, gain, mixed, normed):
    mine = pl.multiple_of(index[2] * half, half)
    total = own[...].astype(jnp.float32) + other[...].astype(jnp.float32)
    rounded = (residual[pl.ds(mine, half), :].astype(jnp.float32) + total).astype(jnp.bfloat16)
    mixed[...] = rounded
    value = rounded.astype(jnp.float32)
    power = jnp.mean(value * value, axis=-1, keepdims=True)
    normed[...] = (value * lax.rsqrt(power + EPSILON) * gain[...]).astype(jnp.bfloat16)


def arrange_kernel(moves, plane, block, index, *refs):
    out = refs[-1]
    z, g = index[0], index[1]
    for p, k, number, source, target, rows in moves:
        place = ((z ^ k) * plane + (g ^ p)) * block + target
        out[pl.ds(pl.multiple_of(place, rows), rows), :] = refs[number][source : source + rows, :]


def lift_kernel(up, *refs):
    rows, hidden, left = refs[:-2], refs[-2], refs[-1]
    half = rows[0].shape[0]
    for r, piece in enumerate(rows):
        left[r * half : (r + 1) * half, :] = piece[...]
    tile = 256
    for n in range(up.shape[1] // tile):
        span = slice(n * tile, (n + 1) * tile)
        active = jnp.maximum(
            jnp.dot(left[...], up[:, span], preferred_element_type=jnp.float32), 0.0
        )
        hidden[:, span] = (active * active).astype(jnp.bfloat16)


def lower_kernel(hidden, down, own, other):
    count, half, width = own.shape
    tile = 512
    for n in range(width // tile):
        span = slice(n * tile, (n + 1) * tile)
        part = lax.dot_general(
            hidden[...],
            down[span, :],
            (((1,), (1,)), ((), ())),
            preferred_element_type=jnp.float32,
        ).astype(jnp.bfloat16)
        for r in range(count):
            rest = (r + count) * half
            own[r, :, span] = part[r * half : (r + 1) * half]
            other[r, :, span] = part[rest : rest + half]


def join_kernel(half, mine, theirs, out):
    core = lax.axis_index("tp")
    out[pl.ds(pl.multiple_of(core * half, half), half), :] = mine[...]
    out[pl.ds(pl.multiple_of((1 - core) * half, half), half), :] = theirs[...]


def fast_body(slots, plane, *arguments):
    (
        residual,
        query_first,
        key_first,
        value_first,
        query_second,
        key_second,
        value_second,
        balance_first,
        balance_second,
        head_gain_first,
        head_gain_second,
        out_first,
        out_second,
        mlp_gain,
        up_weight,
        down_weight,
    ) = arguments
    count = slots * plane
    tokens, width = residual.shape
    half = tokens // 2
    device, core = lax.axis_index("sp"), lax.axis_index("tp")
    z, g = device // plane, device % plane
    index = jnp.stack([z, g, core]).astype(jnp.int32)

    def along(value, k):
        if k == 0:
            return value
        return lax.ppermute(
            value, "sp", [(i, (i // plane ^ k) * plane + i % plane) for i in range(count)]
        )

    def across(value, k):
        if k == 0:
            return value
        return lax.ppermute(value, "sp", [(i, i ^ k) for i in range(count)])

    def swap(value):
        return lax.ppermute(value, "tp", [(0, 1), (1, 0)])

    smem = pl.BlockSpec(memory_space=SMEM)
    hidden = up_weight.shape[1] // slots
    block = up_weight.shape[0]
    sources = (
        key_first,
        key_second.transpose(1, 2, 0),
        value_second.transpose(1, 2, 0),
        value_first,
        query_first,
        query_second.transpose(1, 2, 0),
    )
    packed = pl.pallas_call(
        functools.partial(pack_kernel, slots, plane),
        out_shape=(jax.ShapeDtypeStruct((tokens, 576), jnp.bfloat16),) * slots,
        in_specs=[pl.BlockSpec(memory_space=pltpu.HBM)] * 6,
        out_specs=tuple(vmem_specs(slots)),
        scratch_shapes=[VMEM(source.shape, jnp.bfloat16) for source in sources]
        + [VMEM((slots, tokens, 576), jnp.bfloat16), pltpu.SemaphoreType.DMA((6,))],
        cost_estimate=pl.CostEstimate(flops=10**8, bytes_accessed=10**6, transcendentals=0),
        name="pack",
    )(*sources)
    piece_shape = jax.ShapeDtypeStruct((block, hidden), jnp.bfloat16)
    cuts = pl.pallas_call(
        functools.partial(cut_kernel, slots, plane, hidden),
        out_shape=(jax.ShapeDtypeStruct((2 * block, hidden), jnp.bfloat16),) * (slots - 1)
        + (piece_shape,) * 2,
        in_specs=[pl.BlockSpec(memory_space=pltpu.HBM)] * 2,
        out_specs=tuple(vmem_specs(slots + 1)),
        scratch_shapes=[pltpu.SemaphoreType.DMA((2 * slots,))],
        cost_estimate=pl.CostEstimate(flops=10**8, bytes_accessed=10**6, transcendentals=0),
        name="cut",
    )(up_weight, down_weight)
    early, middle, distant, last_ups, last_downs = cuts
    got = [along(packed[k], k) for k in range(slots)]
    keyval = jnp.stack([piece[:, :384] for piece in got])
    kv_pieces = [across(keyval, p) for p in range(plane - 1)]
    halves = (kv_pieces[2][: slots // 2], kv_pieces[1][slots // 2 :])
    kv_pieces.append(across(halves[0], 1))
    kv_pieces.append(across(halves[1], 2))

    firsts = [across(early, p) for p in range(3)]
    last_up = across(firsts[2][:block], 1)
    last_down = across(firsts[1][block:], 2)

    def gather(arrays):
        mine = jnp.concatenate(arrays, axis=0) if len(arrays) > 1 else arrays[0]
        near = [mine, across(mine, 1), across(mine, 2)]
        blocks = mine.shape[0] // block
        pieces = [
            [(p, near[p], i * block, 0, block) for p in range(3)] for i in range(blocks)
        ]
        split = mine.shape[0] // 2
        rows = math.gcd(block, split)
        for way, low in ((1, 0), (2, split)):
            sent = near[3 - way][low : low + split]
            far = across(sent, way)
            for row in range(low, low + split, rows):
                pieces[row // block].append((3, far, row - low, row % block, rows))
        return pieces

    def arrange(pieces):
        arrays = []
        moves = []
        for p, k, array, *rest in pieces:
            numbers = [i for i, other in enumerate(arrays) if other is array]
            if not numbers:
                numbers = [len(arrays)]
                arrays.append(array)
            moves.append((p, k, numbers[0], *rest))
        return pl.pallas_call(
            functools.partial(arrange_kernel, tuple(moves), plane, block),
            out_shape=jax.ShapeDtypeStruct((count * block, hidden), jnp.bfloat16),
            in_specs=[smem] + vmem_specs(len(arrays)),
            out_specs=pl.BlockSpec(memory_space=VMEM),
            compiler_params=pltpu.CompilerParams(vmem_limit_bytes=16 * 2**20),
            cost_estimate=pl.CostEstimate(flops=10**8, bytes_accessed=10**6, transcendentals=0),
        )(index, *arrays)

    own_up = [(p, 0, firsts[p], 0, 0, block) for p in range(3)]
    own_up.append((3, 0, last_up, 0, 0, block))
    own_down = [(p, 0, firsts[p], block, 0, block) for p in range(3)]
    own_down.append((3, 0, last_down, 0, 0, block))

    def label(k, pieces):
        return [(p, k, *rest) for p, *rest in pieces]

    first_moved = [along(middle, 1), along(last_ups, 3)]
    group = gather(first_moved)
    own_up += label(1, group[0]) + label(3, group[2])
    own_down += label(1, group[1])
    group = gather([along(distant, 2)])
    own_up += label(2, group[0])
    own_down += label(2, group[1])
    own_down += label(3, gather([along(last_downs, 3)])[0])
    up = arrange(own_up)
    down = arrange(own_down)

    sequence = count * tokens
    heads = pl.pallas_call(
        functools.partial(attend_kernel, slots, plane, tokens),
        out_shape=(jax.ShapeDtypeStruct((tokens, 192), jnp.bfloat16),) * slots,
        in_specs=[smem] * 3 + vmem_specs(3 + slots + plane),
        out_specs=tuple(vmem_specs(slots)),
        compiler_params=pltpu.CompilerParams(vmem_limit_bytes=24 * 2**20),
                scratch_shapes=[
            VMEM((slots, tokens, 192), jnp.bfloat16),
            VMEM((sequence, 384), jnp.bfloat16),
            VMEM((2 * tokens, sequence), jnp.float32),
            VMEM((slots, tokens, 192), jnp.bfloat16),
        ],
        cost_estimate=pl.CostEstimate(flops=8 * 10**9, bytes_accessed=2 * 10**6, transcendentals=0),
        name="attend",
    )(
        index,
        balance_first,
        balance_second,
        head_gain_first[None],
        head_gain_second[None],
        *got,
        *kv_pieces,
    )
    pieces = [along(heads[k], k) for k in range(slots)]
    row_shape = jax.ShapeDtypeStruct((half, width), jnp.bfloat16)
    own, other = pl.pallas_call(
        functools.partial(project_kernel, slots, half),
        out_shape=(row_shape, row_shape),
        in_specs=[smem] + vmem_specs(slots + 2),
        out_specs=tuple(vmem_specs(2)),
        scratch_shapes=[VMEM((slots, tokens, 192), jnp.bfloat16)],
        compiler_params=pltpu.CompilerParams(vmem_limit_bytes=16 * 2**20),
                cost_estimate=pl.CostEstimate(flops=2 * 10**9, bytes_accessed=4 * 10**6, transcendentals=0),
        name="project",
    )(index, *pieces, out_first, out_second)
    mixed, normed = pl.pallas_call(
        functools.partial(norm_kernel, half),
        out_shape=(row_shape, row_shape),
        in_specs=[smem] + vmem_specs(4),
        out_specs=tuple(vmem_specs(2)),
        compiler_params=pltpu.CompilerParams(vmem_limit_bytes=8 * 2**20),
                cost_estimate=pl.CostEstimate(flops=10**9, bytes_accessed=10**6, transcendentals=0),
        name="norm",
    )(index, residual, own, swap(other), mlp_gain[None])
    own_rows = [along(normed, k) for k in range(3)]
    own_rows.append(along(own_rows[2], 1))
    other_rows = [swap(piece) for piece in own_rows]
    group = slots // 2
    part_shape = jax.ShapeDtypeStruct((group, half, width), jnp.bfloat16)
    total = None

    def lift(chosen_slots):
        chosen = [own_rows[k] for k in chosen_slots] + [other_rows[k] for k in chosen_slots]
        return pl.pallas_call(
            lift_kernel,
            out_shape=jax.ShapeDtypeStruct((2 * group * half, hidden), jnp.bfloat16),
            in_specs=vmem_specs(1 + 2 * group),
            out_specs=pl.BlockSpec(memory_space=VMEM),
            scratch_shapes=[VMEM((2 * group * half, width), jnp.bfloat16)],
            compiler_params=pltpu.CompilerParams(vmem_limit_bytes=16 * 2**20),
            cost_estimate=pl.CostEstimate(flops=3 * 10**9, bytes_accessed=10**6, transcendentals=0),
        )(up, *chosen)

    def lower(active):
        return pl.pallas_call(
            lower_kernel,
            out_shape=(part_shape, part_shape),
            in_specs=vmem_specs(2),
            out_specs=tuple(vmem_specs(2)),
            compiler_params=pltpu.CompilerParams(vmem_limit_bytes=16 * 2**20),
            cost_estimate=pl.CostEstimate(flops=3 * 10**9, bytes_accessed=10**6, transcendentals=0),
        )(active, down)

    def finish(chosen):
        own, other = lower(lift(chosen))
        other = swap(other)
        summed = own.astype(jnp.float32) + other.astype(jnp.float32)
        return summed[0], summed[1]

    farthest, far = finish((3, 2))
    direct = 128 * round(width * DIRECT / 128)
    sent, far_sent = farthest.astype(jnp.bfloat16), far.astype(jnp.bfloat16)
    passed = along(sent[:, direct:], 1).astype(jnp.float32)
    straight = along(sent[:, :direct], 3).astype(jnp.float32)
    straight = straight + along(far_sent[:, :direct], 2).astype(jnp.float32)
    relayed = along((far[:, direct:] + passed).astype(jnp.bfloat16), 2).astype(jnp.float32)
    near, total = finish((1, 0))
    total = total + along(near.astype(jnp.bfloat16), 1).astype(jnp.float32)
    total = total + jnp.concatenate([straight, relayed], axis=1)
    mine = (mixed.astype(jnp.float32) + total).astype(jnp.bfloat16)
    theirs = swap(mine)
    return pl.pallas_call(
        functools.partial(join_kernel, half),
        out_shape=jax.ShapeDtypeStruct((tokens, width), jnp.bfloat16),
        in_specs=vmem_specs(2),
        out_specs=pl.BlockSpec(memory_space=VMEM),
        compiler_params=pltpu.CompilerParams(vmem_limit_bytes=8 * 2**20),
        cost_estimate=pl.CostEstimate(flops=10**6, bytes_accessed=10**6, transcendentals=0),
        name="join",
    )(mine, theirs)


def dispatch(count, cores, *arguments):
    heads, other_heads = arguments[1].shape[1], arguments[4].shape[1]
    plane = count // heads
    fits = (
        cores == 2
        and heads == other_heads
        and plane == 4
        and heads == 4
        and plane * heads == count
        and arguments[3].shape[2] == 128
        and arguments[6].shape[2] == 64
    )
    if fits:
        return fast_body(heads, plane, *arguments)
    return body(*arguments)


def plan(mesh):
    return functools.partial(dispatch, mesh.shape["sp"], mesh.shape["tp"])


def solution(mesh):
    in_specs = (
        P("sp", None),
        P("sp", "tp", None),
        P("sp", "tp", None),
        P("sp", "tp", None),
        P("sp", "tp", None),
        P("sp", "tp", None),
        P("sp", "tp", None),
        P("tp"),
        P("tp"),
        P(),
        P(),
        P("tp", None),
        P("tp", None),
        P(),
        P("sp", "tp"),
        P("sp", "tp"),
    )
    out_specs = P("sp", None)
    return jax.shard_map(
        plan(mesh), mesh=mesh, in_specs=in_specs, out_specs=out_specs, check_vma=False
    )
```
